32 devices in a mesh: sp: 8 (over z, y), tp: 4 (over x, core).
Axes of the slice: x: 2, y: 2, z: 4, core: 2. Of those that a mesh axis runs over, the one named last changes fastest.
Arguments:
- query: bfloat16 [4096, 1024], P('sp', 'tp'), may hold values from -6 to 6
- key: bfloat16 [4096, 1024], P('sp', 'tp'), may hold values from -6 to 6
- value: bfloat16 [4096, 1024], P('sp', 'tp'), may hold values from -6 to 6
- out_grad: bfloat16 [4096, 1024], P('sp', 'tp'), may hold values from -6 to 6
- query_gain: float32 [64], replicated, may hold values from 0.1 to 1.9
- key_gain: float32 [64], replicated, may hold values from 0.1 to 1.9
- rel_bias: float32 [16, 129], P('tp'), may hold values from -3 to 3
Outputs:
- query_grad: bfloat16 [4096, 1024], P('sp', 'tp')
- key_grad: bfloat16 [4096, 1024], P('sp', 'tp')
- value_grad: bfloat16 [4096, 1024], P('sp', 'tp')
- query_gain_grad: float32 [64], replicated
- key_gain_grad: float32 [64], replicated
- bias_grad: float32 [16, 129], P('tp')
The draws below stay inside these ranges and needn't reach their ends.
All inputs are finite; a program needn't handle non-finite values.
Results may differ from the reference program's by a relative error of at most 0.0095.
Values may be sent and summed in bfloat16 or wider, within the bound.
A program may use at most 64 MiB of HBM per device.

```python
import jax
import jax.numpy as jnp
from jax import lax

H = 16
HD = 64
SEG = 64
PREV = 8
CLIP = 128
TOKENS = 4096
ATT = 1024
TAPS = 129


def block_levels(stream_key, extent, shards, smallest, top_value):
    loudness = 1.0
    for dim, blocks in shards:
        heights = jax.random.uniform(jax.random.fold_in(jax.random.fold_in(stream_key, 6), dim), (blocks,), jnp.float32, smallest / len(shards), top_value / len(shards))
        loudness = loudness * jnp.repeat(jnp.exp(heights), extent[dim] // blocks).reshape((-1,) + (1,) * (len(extent) - 1 - dim))
    return loudness


def noise(key, shape, scale, bound, pieces=(), kind=jnp.bfloat16):
    gain = block_levels(key, shape, pieces, -0.22, 0.18) if pieces else 1.0
    entries = jax.random.normal(key, shape, jnp.float32) * scale * gain
    return jnp.minimum(jnp.maximum(entries, -bound), bound).astype(kind)


def setup_inputs(seed: int = 0) -> dict:
    splits = jax.random.split(jax.random.key(seed), 8)
    return {
        "query": noise(splits[0], (TOKENS, ATT), 1.0, 6.0, ((0, 8), (1, 4))),
        "key": noise(splits[1], (TOKENS, ATT), 1.0, 6.0, ((0, 8), (1, 4))),
        "value": noise(splits[2], (TOKENS, ATT), 1.0, 6.0, ((0, 8), (1, 4))),
        "out_grad": noise(splits[3], (TOKENS, ATT), 1.0, 6.0, ((0, 8), (1, 4))),
        "query_gain": jnp.clip(1.0 + 0.18 * jax.random.normal(splits[4], (HD,), jnp.float32), 0.1, 1.9),
        "key_gain": jnp.clip(1.0 + 0.18 * jax.random.normal(splits[5], (HD,), jnp.float32), 0.1, 1.9),
        "rel_bias": noise(splits[6], (H, TAPS), 0.5, 3.0, ((0, 4),), jnp.float32),
    }


epsilon = 1e-06

def normalize(head_rows, gain_vector):
    widened = head_rows.astype(jnp.float32)
    row_scale = lax.rsqrt(lax.optimization_barrier(jnp.mean(widened * widened, axis=-1, keepdims=True)) + epsilon)
    unit_rows = widened * row_scale
    return (unit_rows, row_scale, (unit_rows * gain_vector).astype(jnp.bfloat16))

def norm_backward(grad_hat, unit_rows, row_scale, gain_vector):
    grad_unit = grad_hat * gain_vector
    inner_mean = lax.optimization_barrier(jnp.mean(grad_unit * unit_rows, axis=-1, keepdims=True))
    return (row_scale * (grad_unit - unit_rows * inner_mean), lax.optimization_barrier(jnp.sum(grad_hat * unit_rows, axis=(0, 1))))

def bias_matrix(table_row, block):
    tap_count = table_row.shape[0]
    position = jnp.arange(3 * block - 1, dtype=jnp.int32)
    distance = jnp.clip(2 * block - 1 - position, 0, tap_count - 1)
    selected = distance[:, None] == jnp.arange(tap_count, dtype=jnp.int32)[None, :]
    diagonal = lax.optimization_barrier(jnp.sum(jnp.where(selected, table_row[None, :], jnp.zeros((), table_row.dtype)), axis=1))
    diagonal = jnp.concatenate([diagonal[block - 1:], jnp.zeros((1,), diagonal.dtype), diagonal[:block - 1]])
    flattened = jnp.tile(diagonal, block)[:block * (3 * block - 1)]
    return flattened.reshape(block, 3 * block - 1)[:, :2 * block]

def tap_totals(score_grad, tap_count):
    block = score_grad.shape[0]
    widened = jnp.pad(score_grad, ((0, 0), (0, block - 1)))
    flattened = jnp.pad(widened.reshape(-1), (0, block))
    columns = lax.optimization_barrier(jnp.sum(flattened.reshape(block, 3 * block), axis=0))
    near_taps = columns[block - tap_count + 2:block + 1][::-1]
    return jnp.concatenate([near_taps, (jnp.sum(columns) - jnp.sum(near_taps))[None]])

def band_mask(block):
    row_index = jnp.arange(block, dtype=jnp.int32)[:, None]
    col_index = jnp.arange(2 * block, dtype=jnp.int32)[None, :]
    return (row_index + block >= col_index) & (col_index // SEG >= row_index // SEG)

def block_gradients(query_block, key_block, value_block, grad_block, bias_block, allowed, score_scale, skip_rows):
    scores = jnp.dot(query_block, key_block.T, preferred_element_type=jnp.float32) * score_scale + bias_block
    normalizer = lax.optimization_barrier(jnp.sum(jnp.where(allowed, jnp.exp(scores), jnp.zeros((), jnp.float32)), axis=1, keepdims=True))
    log_total = jnp.log(normalizer)
    attention = jnp.where(allowed, jnp.exp(scores - log_total), jnp.zeros((), jnp.float32))
    attention_low = attention.astype(jnp.bfloat16)
    output_low = jnp.dot(attention_low, value_block, preferred_element_type=jnp.float32).astype(jnp.bfloat16)
    output_low = lax.optimization_barrier(output_low)
    row_delta = lax.optimization_barrier(jnp.sum(grad_block.astype(jnp.float32) * output_low.astype(jnp.float32), axis=1, keepdims=True))
    attention_grad = jnp.dot(grad_block, value_block.T, preferred_element_type=jnp.float32)
    score_grad = attention * (attention_grad - row_delta)
    score_low = score_grad.astype(jnp.bfloat16)
    query_part = jnp.dot(score_low, key_block, preferred_element_type=jnp.float32) * score_scale
    key_part = jnp.dot(score_low[:, skip_rows:].T, query_block, preferred_element_type=jnp.float32) * score_scale
    value_part = jnp.dot(attention_low[:, skip_rows:].T, grad_block, preferred_element_type=jnp.float32)
    tap_part = tap_totals(score_grad, bias_block.shape[0] * 0 + CLIP + 1)
    return (query_part, key_part, value_part, tap_part, log_total, row_delta)

def reference(query, key, value, out_grad, query_gain, key_gain, rel_bias):
    block = PREV * SEG
    score_scale = HD ** (-0.5)
    shape = (TOKENS, H, HD)
    query_unit, query_scale, query_hat = normalize(query.reshape(shape), query_gain)
    key_unit, key_scale, key_hat = normalize(key.reshape(shape), key_gain)
    padding = jnp.zeros((block, H, HD), jnp.bfloat16)
    key_heads = jnp.concatenate([padding, key_hat]).transpose(1, 0, 2)
    value_heads = jnp.concatenate([padding, value.reshape(shape)]).transpose(1, 0, 2)
    query_heads = query_hat.transpose(1, 0, 2)
    grad_heads = out_grad.reshape(shape).transpose(1, 0, 2)
    inside = band_mask(block)
    later = jnp.arange(2 * block, dtype=jnp.int32)[None, :] >= block
    block_count = TOKENS // block

    def per_head(items):
        query_rows, key_rows, value_rows, grad_rows, table_row = items
        bias_block = bias_matrix(table_row, block)

        def per_block(block_index):
            row_start = (block_index * block).astype(jnp.int32)
            allowed = inside & (later | (block_index > 0))
            query_block = lax.dynamic_slice_in_dim(query_rows, row_start, block, 0)
            key_block = lax.dynamic_slice_in_dim(key_rows, row_start, 2 * block, 0)
            value_block = lax.dynamic_slice_in_dim(value_rows, row_start, 2 * block, 0)
            grad_block = lax.dynamic_slice_in_dim(grad_rows, row_start, block, 0)
            results = block_gradients(query_block, key_block, value_block, grad_block, bias_block, allowed, score_scale, 0)
            return (results[0], results[1], results[2], results[3])
        query_part, key_part, value_part, tap_part = lax.map(per_block, jnp.arange(block_count, dtype=jnp.int32))
        key_sum = jnp.pad(key_part[:, :block].reshape(-1, HD), ((0, block), (0, 0))) + jnp.pad(key_part[:, block:].reshape(-1, HD), ((block, 0), (0, 0)))
        value_sum = jnp.pad(value_part[:, :block].reshape(-1, HD), ((0, block), (0, 0))) + jnp.pad(value_part[:, block:].reshape(-1, HD), ((block, 0), (0, 0)))
        return (query_part.reshape(-1, HD), key_sum[block:], value_sum[block:], lax.optimization_barrier(jnp.sum(tap_part, axis=0)))
    query_hat_grad, key_hat_grad, value_sum, bias_grad = lax.map(per_head, (query_heads, key_heads, value_heads, grad_heads, rel_bias))
    query_grad, query_gain_grad = norm_backward(query_hat_grad.transpose(1, 0, 2), query_unit, query_scale, query_gain)
    key_grad, key_gain_grad = norm_backward(key_hat_grad.transpose(1, 0, 2), key_unit, key_scale, key_gain)
    value_grad = value_sum.transpose(1, 0, 2).reshape(TOKENS, ATT)
    return (query_grad.reshape(TOKENS, ATT).astype(jnp.bfloat16), key_grad.reshape(TOKENS, ATT).astype(jnp.bfloat16), value_grad.astype(jnp.bfloat16), query_gain_grad, key_gain_grad, bias_grad)
```

```python
import functools

import jax
import jax.numpy as jnp
from jax import lax
from jax.experimental import pallas as pl
from jax.experimental.pallas import tpu as pltpu
from jax.sharding import PartitionSpec as P

CLIP = 128
TILE = 128
LANES = 128
WIDE = 2 * TILE
EPSILON = 1e-06
LOG2E = 1.4426950408889634
MASKED = -1e30
MESH = pl.DeviceIdType.MESH
NT = (((1,), (1,)), ((), ()))
NN = (((1,), (0,)), ((), ()))


def dot(a, b, dims=NN):
    return lax.dot_general(a, b, dims, preferred_element_type=jnp.float32)


def iota(shape, axis):
    return lax.broadcasted_iota(jnp.int32, shape, axis)


def half_mean(x):
    low = iota(x.shape, 1) < LANES // 2
    first = jnp.sum(jnp.where(low, x, 0.0), axis=1, keepdims=True)
    second = jnp.sum(jnp.where(low, 0.0, x), axis=1, keepdims=True)
    return jnp.where(low, first, second) * (2.0 / LANES)


def unit_of(x):
    scale = lax.rsqrt(half_mean(x * x) + EPSILON)
    return x * scale, scale


def skew(x, left):
    row = iota(x.shape, 0)
    for bit in range(7):
        step = 1 << bit
        moved = pltpu.roll(x, LANES - step if left else step, 1)
        x = jnp.where((row & step) != 0, moved, x)
    return x


def kernel(
    axis_sizes,
    head_width,
    q_hbm,
    k_hbm,
    v_hbm,
    g_hbm,
    q_gain_ref,
    k_gain_ref,
    bias_ref,
    q_out_hbm,
    k_out_hbm,
    v_out_hbm,
    q_gain_out,
    k_gain_out,
    bias_out,
    q_ref,
    k_ref,
    v_ref,
    g_ref,
    q_out,
    k_out,
    v_out,
    next_q,
    next_g,
    stat_send,
    stat_recv,
    next_stat,
    dq_send,
    dq_recv,
    k_hat,
    k_turned,
    own_q,
    own_g,
    far_q,
    far_g,
    own_e,
    own_p,
    far_e,
    far_p,
    dk,
    dv,
    dq_own,
    near_bias,
    taps,
    totals,
    own_stat,
    q_unit,
    q_scale,
    next_unit,
    k_unit,
    k_scale,
    gain_part,
    message,
    gathered,
    gain_message,
    gain_gathered,
    in_send_sem,
    in_recv_sem,
    stat_send_sem,
    stat_recv_sem,
    own_send_sem,
    own_recv_sem,
    dq_send_sem,
    dq_recv_sem,
    sum_send_sem,
    sum_recv_sem,
    gain_send_sem,
    gain_recv_sem,
    load_sem,
    store_sem,
):
    n_sp, n_tp = axis_sizes
    rows, width = q_hbm.shape
    tiles = rows // TILE
    pairs = width // LANES
    heads = 2 * pairs
    score_scale = head_width ** (-0.5)
    me = lax.axis_index("sp")
    me_tp = lax.axis_index("tp")
    has_prev = me > 0
    has_next = me < n_sp - 1
    before = jnp.maximum(me - 1, 0)
    after = jnp.minimum(me + 1, n_sp - 1)

    def span(t):
        return slice(t * TILE, (t + 1) * TILE)

    def pair_lanes(p):
        return slice(p * LANES, (p + 1) * LANES)

    def copy(src, dst, send, recv, target):
        return pltpu.make_async_remote_copy(
            src_ref=src,
            dst_ref=dst,
            send_sem=send,
            recv_sem=recv,
            device_id={"sp": target},
            device_id_type=MESH,
        )

    def in_copies(t):
        return (
            copy(q_ref.at[span(t)], next_q.at[span(t)], in_send_sem.at[2 * t], in_recv_sem.at[2 * t], before),
            copy(g_ref.at[span(t)], next_g.at[span(t)], in_send_sem.at[2 * t + 1], in_recv_sem.at[2 * t + 1], before),
        )

    def stat_copy(t):
        return copy(stat_send.at[t], stat_recv.at[t], stat_send_sem.at[t], stat_recv_sem.at[t], after)

    def own_copy():
        return copy(own_stat, next_stat, own_send_sem.at[0], own_recv_sem.at[0], before)

    def dq_copy(t):
        return copy(dq_send.at[t], dq_recv.at[t], dq_send_sem.at[t], dq_recv_sem.at[t], after)

    def loop(count, body):
        def step(i, carry):
            body(i + 1)
            return carry

        lax.fori_loop(0, count - 1, step, 0)

    def sp_peer(k):
        return lax.rem(me + k, n_sp)

    def tp_peer(k):
        return lax.rem(me_tp + k, n_tp)

    barrier = pltpu.get_barrier_semaphore()

    def greet(target):
        pl.semaphore_signal(barrier, inc=1, device_id=target, device_id_type=MESH)

    loop(n_sp, lambda k: greet({"sp": sp_peer(k)}))
    loop(n_tp, lambda k: greet({"tp": tp_peer(k)}))
    moves = ((q_hbm, q_ref), (g_hbm, g_ref), (k_hbm, k_ref), (v_hbm, v_ref))
    loads = [pltpu.make_async_copy(a, b, load_sem.at[i]) for i, (a, b) in enumerate(moves)]
    moves = ((k_out, k_out_hbm), (v_out, v_out_hbm), (q_out, q_out_hbm))
    stores = [pltpu.make_async_copy(a, b, store_sem.at[i]) for i, (a, b) in enumerate(moves)]
    for c in loads:
        c.start()
    pl.semaphore_wait(barrier, n_sp + n_tp - 2)
    loads[0].wait()
    loads[1].wait()

    in_order = [c for t in range(tiles) for c in in_copies(t)]
    ahead = min(3, len(in_order))

    @pl.when(has_prev)
    def _():
        for c in in_order[:ahead]:
            c.start()

    loads[2].wait()
    loads[3].wait()
    q_gain = jnp.concatenate([q_gain_ref[...]] * 2, axis=1)
    k_gain = jnp.concatenate([k_gain_ref[...]] * 2, axis=1)
    low_lane = iota((TILE, LANES), 1) < LANES // 2

    def split_heads(x):
        first = jnp.where(low_lane, x, 0.0)
        second = jnp.where(low_lane, 0.0, x)
        return jnp.concatenate([first, second], axis=0).astype(jnp.bfloat16)

    def load_queries(q_from, g_from, t, q_to, g_to, unit_to, scale_to):
        for p in range(pairs):
            x = q_from[span(t), pair_lanes(p)].astype(jnp.float32)
            unit, scale = unit_of(x)
            unit_to[p, span(t)] = unit
            if scale_to is not None:
                scale_to[p, span(t)] = scale
            q_to[p, t] = split_heads(unit * q_gain)
            g_to[p, t] = split_heads(g_from[span(t), pair_lanes(p)].astype(jnp.float32))

    key_at = iota((TILE, WIDE), 0)
    query_at = iota((TILE, WIDE), 1) % TILE
    causal = query_at >= key_at
    far_bias = jnp.where((key_at // 64) >= (query_at // 64), 0.0, MASKED)

    for p in range(pairs):
        for t in range(tiles):
            x = k_ref[span(t), pair_lanes(p)].astype(jnp.float32)
            unit, scale = unit_of(x)
            k_unit[p, span(t)] = unit
            k_scale[p, span(t)] = scale
            hat = unit * k_gain
            k_hat[p, span(t)] = hat.astype(jnp.bfloat16)
            k_turned[p, :, span(t)] = hat.T.astype(jnp.bfloat16)
        sheets = []
        for h in (2 * p, 2 * p + 1):
            table = (bias_ref[h : h + 1, 0:CLIP] - bias_ref[h : h + 1, CLIP : CLIP + 1]) * LOG2E
            sheets.append(skew(jnp.broadcast_to(table, (TILE, LANES)), False))
        near_bias[p] = jnp.concatenate(sheets, axis=1)
    dk[...] = jnp.zeros_like(dk)
    dv[...] = jnp.zeros_like(dv)
    taps[...] = jnp.zeros_like(taps)
    totals[...] = jnp.zeros_like(totals)
    gain_part[...] = jnp.zeros_like(gain_part)

    def forward(p, t, start, stop, kinds, q_from, g_from, e_to, p_to):
        keys = slice(start * TILE, stop * TILE)
        raw = dot(k_hat[p, keys], q_from[p, t], NT)
        grad = dot(v_ref[keys, pair_lanes(p)], g_from[p, t], NT)
        total = jnp.zeros((1, WIDE), jnp.float32)
        inner = jnp.zeros((1, WIDE), jnp.float32)
        for c in range(start, stop):
            here = slice((c - start) * TILE, (c - start + 1) * TILE)
            s = raw[here] * (score_scale * LOG2E)
            kind = kinds.get(c)
            if kind == "diagonal":
                s = jnp.where(causal, s + near_bias[p], MASKED)
            elif kind == "below":
                s = s + jnp.where(causal, 0.0, near_bias[p])
            elif kind == "far":
                s = s + far_bias
            e = jnp.exp2(s)
            dp = grad[here]
            e_to[p, t, span(c)] = e
            p_to[p, t, span(c)] = dp
            total = total + jnp.sum(e, axis=0, keepdims=True)
            inner = inner + jnp.sum(e * dp, axis=0, keepdims=True)
        return total, inner

    def backward(p, t, start, stop, kinds, q_from, g_from, e_from, p_from, inverse, delta):
        keys = slice(start * TILE, stop * TILE)
        attention = e_from[p, t, keys] * inverse
        grad = attention * (p_from[p, t, keys] - delta)
        attention_low = attention.astype(jnp.bfloat16)
        grad_low = grad.astype(jnp.bfloat16)
        dv[p, keys] += dot(attention_low, g_from[p, t])
        dk[p, keys] += dot(grad_low, q_from[p, t])
        turned = dot(k_turned[p, :, keys], grad_low)
        totals[p : p + 1] += jnp.sum(grad, axis=0, keepdims=True)
        for c, kind in kinds.items():
            part = grad[(c - start) * TILE : (c - start + 1) * TILE]
            if kind == "diagonal":
                taps[p] += part
            elif kind == "below":
                taps[p] += jnp.where(causal, 0.0, part)
        upper = iota((LANES, TILE), 0) < LANES // 2
        return jnp.where(upper, turned[:, :TILE], turned[:, TILE:]).T

    def own_kinds(t):
        kinds = {t: "diagonal"}
        if t > 0:
            kinds[t - 1] = "below"
        return kinds

    def far_forward_kinds(t):
        kinds = {t: "far"}
        if t == 0:
            kinds[tiles - 1] = "below"
        return kinds

    def stat_row(p, t):
        return 2 * (t * pairs + p)

    def normalizers(p, t, own, far):
        row = stat_row(p, t)
        total = own[row : row + 1] + far[t, 2 * p : 2 * p + 1]
        inner = own[row + 1 : row + 2] + far[t, 2 * p + 1 : 2 * p + 2]
        inverse = 1.0 / total
        return inverse, inner * inverse

    for t in range(tiles):
        load_queries(q_ref, g_ref, t, own_q, own_g, q_unit, q_scale)
        for p in range(pairs):
            total, inner = forward(p, t, 0, t + 1, own_kinds(t), own_q, own_g, own_e, own_p)
            row = stat_row(p, t)
            own_stat[row : row + 1] = total
            own_stat[row + 1 : row + 2] = inner

    @pl.when(has_prev)
    def _():
        own_copy().start()
        for c in in_order[ahead:]:
            c.start()

    @pl.when(jnp.logical_not(has_prev))
    def _():
        stat_recv[...] = jnp.zeros_like(stat_recv)
        dq_recv[...] = jnp.zeros_like(dq_recv)

    def far_forward(t):
        @pl.when(has_next)
        def _():
            for c in in_copies(t):
                c.wait_recv()
            load_queries(next_q, next_g, t, far_q, far_g, next_unit, None)
            for p in range(pairs):
                total, inner = forward(
                    p, t, t, tiles, far_forward_kinds(t), far_q, far_g, far_e, far_p
                )
                stat_send[t, 2 * p : 2 * p + 1] = total
                stat_send[t, 2 * p + 1 : 2 * p + 2] = inner
            stat_copy(t).start()

    def far_backward(t):
        @pl.when(has_next)
        def _():
            if t == 0:
                own_copy().wait_recv()
            for p in range(pairs):
                inverse, delta = normalizers(p, t, next_stat, stat_send)
                part = backward(
                    p, t, t, tiles, far_forward_kinds(t), far_q, far_g, far_e, far_p, inverse, delta
                )
                dq_send[t, :, pair_lanes(p)] = part.astype(jnp.bfloat16)
                gain_part[...] += jnp.sum(part * next_unit[p, span(t)], axis=0, keepdims=True)

    def dq_start(ts):
        @pl.when(has_next)
        def _():
            for t in ts:
                dq_copy(t).start()

    def own_backward(t):
        @pl.when(has_prev)
        def _():
            stat_copy(t).wait_recv()

        for p in range(pairs):
            inverse, delta = normalizers(p, t, own_stat, stat_recv)
            part = backward(
                p, t, 0, t + 1, own_kinds(t), own_q, own_g, own_e, own_p, inverse, delta
            )
            dq_own[p, span(t)] = part
            gain_part[...] += jnp.sum(part * q_unit[p, span(t)], axis=0, keepdims=True)

    for t in range(tiles):
        far_forward(t)
        if t < tiles - 1:
            far_backward(t)
    dq_start(range(tiles - 1))
    far_backward(tiles - 1)
    dq_start(range(tiles - 1, tiles))
    for t in range(tiles):
        own_backward(t)

    k_part = jnp.zeros((1, LANES), jnp.float32)
    for p in range(pairs):
        k_part = k_part + jnp.sum(dk[p] * k_unit[p], axis=0, keepdims=True)

    gain_row = message.shape[0] - 8
    message[...] = jnp.zeros_like(message)
    for h in range(heads):
        lanes = slice((h % 2) * TILE, (h % 2 + 1) * TILE)
        row = jnp.sum(skew(taps[h // 2, :, lanes], True), axis=0, keepdims=True)
        rest = jnp.sum(totals[h // 2 : h // 2 + 1, lanes], axis=1, keepdims=True) - jnp.sum(
            row, axis=1, keepdims=True
        )
        message[h : h + 1] = row
        message[heads + h : heads + h + 1] = jnp.broadcast_to(rest, (1, LANES))
    message[gain_row : gain_row + 1] = gain_part[...] * score_scale
    message[gain_row + 1 : gain_row + 2] = k_part * score_scale

    def sum_copy(k, slot, target):
        return copy(message, gathered.at[slot], sum_send_sem.at[k], sum_recv_sem.at[slot], target)

    loop(n_sp, lambda k: sum_copy(k, me, sp_peer(k)).start())
    gathered[me] = message[...]

    def norm_backward(unit, scale, grad_hat, gain):
        grad_unit = grad_hat * gain
        inner = half_mean(grad_unit * unit)
        return (scale * (grad_unit - unit * inner)).astype(jnp.bfloat16)

    for p in range(pairs):
        for t in range(tiles):
            here = (p, span(t))
            k_out[span(t), pair_lanes(p)] = norm_backward(
                k_unit[here], k_scale[here], dk[here] * score_scale, k_gain
            )
            v_out[span(t), pair_lanes(p)] = dv[here].astype(jnp.bfloat16)

    stores[0].start()
    stores[1].start()

    for t in range(tiles):

        @pl.when(has_prev)
        def _():
            dq_copy(t).wait_recv()

        for p in range(pairs):
            here = (p, span(t))
            grad_hat = (dq_own[here] + dq_recv[t, :, pair_lanes(p)].astype(jnp.float32)) * score_scale
            q_out[span(t), pair_lanes(p)] = norm_backward(
                q_unit[here], q_scale[here], grad_hat, q_gain
            )

    stores[2].start()
    loop(n_sp, lambda k: sum_copy(k, sp_peer(k), sp_peer(k)).wait_recv())
    summed = jnp.sum(gathered[...], axis=0)
    for h in range(heads):
        bias_out[h : h + 1, 0:CLIP] = summed[h : h + 1]
        bias_out[h : h + 1, CLIP : CLIP + 1] = summed[heads + h : heads + h + 1, 0:1]
    gain_message[...] = summed[gain_row:]

    def gain_copy(k, slot):
        return pltpu.make_async_remote_copy(
            src_ref=gain_message,
            dst_ref=gain_gathered.at[slot],
            send_sem=gain_send_sem.at[k],
            recv_sem=gain_recv_sem.at[slot],
            device_id={"tp": tp_peer(k)},
            device_id_type=MESH,
        )

    loop(n_tp, lambda k: gain_copy(k, me_tp).start())
    gain_gathered[me_tp] = gain_message[...]
    loop(n_tp, lambda k: gain_copy(k, tp_peer(k)).wait_recv())
    gains = jnp.sum(gain_gathered[...], axis=0)
    gains = gains + pltpu.roll(gains, LANES // 2, 1)
    q_gain_out[...] = gains[0:1, 0 : LANES // 2]
    k_gain_out[...] = gains[1:2, 0 : LANES // 2]

    for c in stores:
        c.wait()
    loop(n_sp, lambda k: sum_copy(k, me, sp_peer(k)).wait_send())
    loop(n_tp, lambda k: gain_copy(k, me_tp).wait_send())

    @pl.when(has_prev)
    def _():
        own_copy().wait_send()
        for c in in_order:
            c.wait_send()

    @pl.when(has_next)
    def _():
        for t in range(tiles):
            stat_copy(t).wait_send()
            dq_copy(t).wait_send()


def place(*refs):
    half = len(refs) // 2
    for source, target in zip(refs[:half], refs[half:]):
        target[...] = source[...]


def per_device(axis_sizes, query, key, value, out_grad, query_gain, key_gain, rel_bias):
    n_sp, n_tp = axis_sizes
    rows, width = query.shape
    heads, taps = rel_bias.shape
    head_width = width // heads
    tiles = rows // TILE
    pairs = width // LANES
    low, full = jnp.bfloat16, jnp.float32
    message_rows = -(-2 * heads // 8) * 8 + 8
    stat_rows = -(-2 * pairs // 8) * 8
    vmem = pl.BlockSpec(memory_space=pltpu.VMEM)
    anywhere = pl.BlockSpec(memory_space=pl.ANY)
    stat = pltpu.VMEM((tiles, stat_rows, WIDE), full)
    sums = pltpu.VMEM((-(-2 * pairs * tiles // 8) * 8, WIDE), full)
    wide = pltpu.VMEM((pairs, tiles, WIDE, LANES), low)
    square = pltpu.VMEM((pairs, tiles, rows, WIDE), full)
    units = pltpu.VMEM((pairs, rows, LANES), full)
    dma = pltpu.SemaphoreType.DMA
    results = pl.pallas_call(
        functools.partial(kernel, axis_sizes, head_width),
        out_shape=(
            jax.ShapeDtypeStruct((rows, width), low),
            jax.ShapeDtypeStruct((rows, width), low),
            jax.ShapeDtypeStruct((rows, width), low),
            jax.ShapeDtypeStruct((1, head_width), full),
            jax.ShapeDtypeStruct((1, head_width), full),
            jax.ShapeDtypeStruct((heads, taps), full),
        ),
        in_specs=[anywhere] * 4 + [vmem] * 3,
        out_specs=(anywhere,) * 3 + (vmem,) * 3,
        scratch_shapes=[pltpu.VMEM((rows, width), low)] * 7
        + [
            pltpu.VMEM((rows, width), low),
            pltpu.VMEM((rows, width), low),
            stat,
            stat,
            sums,
            pltpu.VMEM((tiles, TILE, width), low),
            pltpu.VMEM((tiles, TILE, width), low),
            pltpu.VMEM((pairs, rows, LANES), low),
            pltpu.VMEM((pairs, LANES, rows), low),
            wide,
            wide,
            wide,
            wide,
            square,
            square,
            square,
            square,
            pltpu.VMEM((pairs, rows, LANES), full),
            pltpu.VMEM((pairs, rows, LANES), full),
            pltpu.VMEM((pairs, rows, LANES), full),
            pltpu.VMEM((pairs, TILE, WIDE), full),
            pltpu.VMEM((pairs, TILE, WIDE), full),
            pltpu.VMEM((8, WIDE), full),
            sums,
            units,
            units,
            units,
            units,
            units,
            pltpu.VMEM((1, LANES), full),
            pltpu.VMEM((message_rows, LANES), full),
            pltpu.VMEM((n_sp, message_rows, LANES), full),
            pltpu.VMEM((8, LANES), full),
            pltpu.VMEM((n_tp, 8, LANES), full),
            dma((2 * tiles,)),
            dma((2 * tiles,)),
            dma((tiles,)),
            dma((tiles,)),
            dma((1,)),
            dma((1,)),
            dma((tiles,)),
            dma((tiles,)),
            dma((n_sp,)),
            dma((n_sp,)),
            dma((n_tp,)),
            dma((n_tp,)),
            dma((4,)),
            dma((3,)),
        ],
        compiler_params=pltpu.CompilerParams(has_side_effects=True, collective_id=0),
    )(query, key, value, out_grad, query_gain.reshape(1, -1), key_gain.reshape(1, -1), rel_bias)
    query_grad, key_grad, value_grad, query_gain_grad, key_gain_grad, bias_grad = pl.pallas_call(
        place,
        out_shape=tuple(jax.ShapeDtypeStruct(x.shape, x.dtype) for x in results),
        in_specs=[vmem] * 6,
        out_specs=(vmem,) * 6,
    )(*results)
    return (
        query_grad,
        key_grad,
        value_grad,
        query_gain_grad.reshape(-1),
        key_gain_grad.reshape(-1),
        bias_grad,
    )


def solution(mesh):
    axis_sizes = (mesh.shape["sp"], mesh.shape["tp"])
    placed = (P("sp", "tp"), P("sp", "tp"), P("sp", "tp"), P("sp", "tp"), P(), P(), P("tp", None))
    return jax.shard_map(
        functools.partial(per_device, axis_sizes),
        mesh=mesh,
        in_specs=placed,
        out_specs=(P("sp", "tp"), P("sp", "tp"), P("sp", "tp"), P(), P(), P("tp", None)),
        check_vma=False,
    )
```

```python
import functools

import jax
import jax.numpy as jnp
from jax import lax
from jax.experimental import pallas as pl
from jax.experimental.pallas import tpu as pltpu
from jax.sharding import PartitionSpec as P

CLIP = 128
TILE = 128
LANES = 128
WIDE = 2 * TILE
EPSILON = 1e-06
LOG2E = 1.4426950408889634
MASKED = -1e30
MAIN_VMEM = 48 * 1024 * 1024
PLACE_VMEM = 4 * 1024 * 1024
MESH = pl.DeviceIdType.MESH
NT = (((1,), (1,)), ((), ()))
NN = (((1,), (0,)), ((), ()))


def dot(a, b, dims=NN):
    return lax.dot_general(a, b, dims, preferred_element_type=jnp.float32)


def iota(shape, axis):
    return lax.broadcasted_iota(jnp.int32, shape, axis)


def half_mean(x):
    low = iota(x.shape, 1) < LANES // 2
    first = jnp.sum(jnp.where(low, x, 0.0), axis=1, keepdims=True)
    second = jnp.sum(jnp.where(low, 0.0, x), axis=1, keepdims=True)
    return jnp.where(low, first, second) * (2.0 / LANES)


def unit_of(x):
    scale = lax.rsqrt(half_mean(x * x) + EPSILON)
    return x * scale, scale


def skew(x, left):
    row = iota(x.shape, 0)
    for bit in range(7):
        step = 1 << bit
        moved = pltpu.roll(x, LANES - step if left else step, 1)
        x = jnp.where((row & step) != 0, moved, x)
    return x


def kernel(
    axis_sizes,
    head_width,
    q_hbm,
    k_hbm,
    v_hbm,
    g_hbm,
    q_gain_hbm,
    k_gain_hbm,
    bias_hbm,
    q_out,
    k_out,
    v_out,
    q_gain_out,
    k_gain_out,
    bias_out,
    q_ref,
    k_ref,
    v_ref,
    g_ref,
    q_gain_ref,
    k_gain_ref,
    bias_ref,
    next_q,
    next_g,
    stat_send,
    stat_recv,
    next_stat,
    dq_send,
    dq_recv,
    k_hat,
    k_turned,
    own_q,
    own_g,
    far_q,
    far_g,
    own_e,
    own_p,
    far_e,
    far_p,
    dk,
    dv,
    dq_own,
    near_bias,
    taps,
    totals,
    own_stat,
    q_unit,
    q_scale,
    next_unit,
    k_unit,
    k_scale,
    gain_part,
    message,
    gathered,
    gain_message,
    gain_gathered,
    in_send_sem,
    in_recv_sem,
    stat_send_sem,
    stat_recv_sem,
    own_send_sem,
    own_recv_sem,
    dq_send_sem,
    dq_recv_sem,
    sum_send_sem,
    sum_recv_sem,
    gain_send_sem,
    gain_recv_sem,
    load_sem,
    met_sem,
):
    n_sp, n_tp = axis_sizes
    rows, width = q_hbm.shape
    tiles = rows // TILE
    pairs = width // LANES
    heads = 2 * pairs
    score_scale = head_width ** (-0.5)
    me = lax.axis_index("sp")
    me_tp = lax.axis_index("tp")
    has_prev = me > 0
    has_next = me < n_sp - 1
    before = jnp.maximum(me - 1, 0)
    after = jnp.minimum(me + 1, n_sp - 1)

    def span(t):
        return slice(t * TILE, (t + 1) * TILE)

    def pair_lanes(p):
        return slice(p * LANES, (p + 1) * LANES)

    def copy(src, dst, send, recv, target):
        return pltpu.make_async_remote_copy(
            src_ref=src,
            dst_ref=dst,
            send_sem=send,
            recv_sem=recv,
            device_id={"sp": target},
            device_id_type=MESH,
        )

    def in_copies(t):
        return (
            copy(q_ref.at[span(t)], next_q.at[span(t)], in_send_sem.at[2 * t], in_recv_sem.at[2 * t], before),
            copy(g_ref.at[span(t)], next_g.at[span(t)], in_send_sem.at[2 * t + 1], in_recv_sem.at[2 * t + 1], before),
        )

    def stat_copy(t):
        return copy(stat_send.at[t], stat_recv.at[t], stat_send_sem.at[t], stat_recv_sem.at[t], after)

    def own_copy():
        return copy(own_stat, next_stat, own_send_sem.at[0], own_recv_sem.at[0], before)

    def dq_copy(t):
        return copy(dq_send.at[t], dq_recv.at[t], dq_send_sem.at[t], dq_recv_sem.at[t], after)

    def loop(count, body):
        def step(i, carry):
            body(i + 1)
            return carry

        lax.fori_loop(0, count - 1, step, 0)

    def sp_peer(k):
        return lax.rem(me + k, n_sp)

    def tp_peer(k):
        return lax.rem(me_tp + k, n_tp)

    everyone = n_sp * n_tp
    me_flat = me * n_tp + me_tp

    def flat_peer(k):
        return lax.rem(me_flat + k, everyone)

    barrier = pltpu.get_barrier_semaphore()

    def greet(target):
        pl.semaphore_signal(barrier, inc=1, device_id=target, device_id_type=MESH)

    pl.when(has_prev)(lambda: greet({"sp": before}))
    pl.when(has_next)(lambda: greet({"sp": after}))
    loop(n_tp, lambda k: greet({"tp": tp_peer(k)}))
    moves = (
        (q_hbm, q_ref),
        (g_hbm, g_ref),
        (k_hbm, k_ref),
        (v_hbm, v_ref),
        (q_gain_hbm, q_gain_ref),
        (k_gain_hbm, k_gain_ref),
        (bias_hbm, bias_ref),
    )
    loads = [pltpu.make_async_copy(a, b, load_sem.at[i]) for i, (a, b) in enumerate(moves)]
    for c in loads:
        c.start()
    pl.semaphore_wait(barrier, has_prev.astype(jnp.int32) + has_next.astype(jnp.int32) + n_tp - 1)
    rounds = met_sem.shape[0]

    def round_signal(r):
        for ok, target in ((me >= 1 << r, me - (1 << r)), (me + (1 << r) < n_sp, me + (1 << r))):

            @pl.when(ok)
            def _():
                pl.semaphore_signal(
                    met_sem.at[r], inc=1, device_id={"sp": target}, device_id_type=MESH
                )

    def round_wait(r):
        count = (me >= 1 << r).astype(jnp.int32) + (me + (1 << r) < n_sp).astype(jnp.int32)
        pl.semaphore_wait(met_sem.at[r], count)

    def meet(r):
        if r < rounds:
            round_wait(r)
        if r + 1 < rounds:
            round_signal(r + 1)

    round_signal(0)
    loads[0].wait()
    loads[1].wait()

    in_order = [c for t in range(tiles) for c in in_copies(t)]
    ahead = min(3, len(in_order))

    @pl.when(has_prev)
    def _():
        for c in in_order[:ahead]:
            c.start()

    for c in loads[2:]:
        c.wait()
    q_gain = jnp.concatenate([q_gain_ref[...]] * 2, axis=1)
    k_gain = jnp.concatenate([k_gain_ref[...]] * 2, axis=1)
    low_lane = iota((TILE, LANES), 1) < LANES // 2

    def split_heads(x):
        first = jnp.where(low_lane, x, 0.0)
        second = jnp.where(low_lane, 0.0, x)
        return jnp.concatenate([first, second], axis=0).astype(jnp.bfloat16)

    def load_queries(q_from, g_from, t, q_to, g_to, unit_to, scale_to):
        for p in range(pairs):
            x = q_from[span(t), pair_lanes(p)].astype(jnp.float32)
            unit, scale = unit_of(x)
            unit_to[p, span(t)] = unit
            if scale_to is not None:
                scale_to[p, span(t)] = scale
            q_to[p, t] = split_heads(unit * q_gain)
            g_to[p, t] = split_heads(g_from[span(t), pair_lanes(p)].astype(jnp.float32))

    key_at = iota((TILE, WIDE), 0)
    query_at = iota((TILE, WIDE), 1) % TILE
    causal = query_at >= key_at
    far_bias = jnp.where((key_at // 64) >= (query_at // 64), 0.0, MASKED)

    for p in range(pairs):
        for t in range(tiles):
            x = k_ref[span(t), pair_lanes(p)].astype(jnp.float32)
            unit, scale = unit_of(x)
            k_unit[p, span(t)] = unit
            k_scale[p, span(t)] = scale
            hat = unit * k_gain
            k_hat[p, span(t)] = hat.astype(jnp.bfloat16)
            k_turned[p, :, span(t)] = hat.T.astype(jnp.bfloat16)
        sheets = []
        for h in (2 * p, 2 * p + 1):
            table = (bias_ref[h : h + 1, 0:CLIP] - bias_ref[h : h + 1, CLIP : CLIP + 1]) * LOG2E
            sheets.append(skew(jnp.broadcast_to(table, (TILE, LANES)), False))
        near_bias[p] = jnp.concatenate(sheets, axis=1)
    dk[...] = jnp.zeros_like(dk)
    dv[...] = jnp.zeros_like(dv)
    taps[...] = jnp.zeros_like(taps)
    totals[...] = jnp.zeros_like(totals)
    gain_part[...] = jnp.zeros_like(gain_part)

    def forward(p, t, start, stop, kinds, q_from, g_from, e_to, p_to):
        keys = slice(start * TILE, stop * TILE)
        raw = dot(k_hat[p, keys], q_from[p, t], NT)
        grad = dot(v_ref[keys, pair_lanes(p)], g_from[p, t], NT)
        total = jnp.zeros((1, WIDE), jnp.float32)
        inner = jnp.zeros((1, WIDE), jnp.float32)
        for c in range(start, stop):
            here = slice((c - start) * TILE, (c - start + 1) * TILE)
            s = raw[here] * (score_scale * LOG2E)
            kind = kinds.get(c)
            if kind == "diagonal":
                s = jnp.where(causal, s + near_bias[p], MASKED)
            elif kind == "below":
                s = s + jnp.where(causal, 0.0, near_bias[p])
            elif kind == "far":
                s = s + far_bias
            e = jnp.exp2(s)
            dp = grad[here]
            e_to[p, t, span(c)] = e
            p_to[p, t, span(c)] = dp
            total = total + jnp.sum(e, axis=0, keepdims=True)
            inner = inner + jnp.sum(e * dp, axis=0, keepdims=True)
        return total, inner

    def backward(p, t, start, stop, kinds, q_from, g_from, e_from, p_from, inverse, delta):
        keys = slice(start * TILE, stop * TILE)
        attention = e_from[p, t, keys] * inverse
        grad = attention * (p_from[p, t, keys] - delta)
        attention_low = attention.astype(jnp.bfloat16)
        grad_low = grad.astype(jnp.bfloat16)
        dv[p, keys] += dot(attention_low, g_from[p, t])
        dk[p, keys] += dot(grad_low, q_from[p, t])
        turned = dot(k_turned[p, :, keys], grad_low)
        totals[p : p + 1] += jnp.sum(grad, axis=0, keepdims=True)
        for c, kind in kinds.items():
            part = grad[(c - start) * TILE : (c - start + 1) * TILE]
            if kind == "diagonal":
                taps[p] += part
            elif kind == "below":
                taps[p] += jnp.where(causal, 0.0, part)
        upper = iota((LANES, TILE), 0) < LANES // 2
        return jnp.where(upper, turned[:, :TILE], turned[:, TILE:]).T

    def own_kinds(t):
        kinds = {t: "diagonal"}
        if t > 0:
            kinds[t - 1] = "below"
        return kinds

    def far_forward_kinds(t):
        kinds = {t: "far"}
        if t == 0:
            kinds[tiles - 1] = "below"
        return kinds

    def stat_row(p, t):
        return 2 * (t * pairs + p)

    def normalizers(p, t, own, far):
        row = stat_row(p, t)
        total = own[row : row + 1] + far[t, 2 * p : 2 * p + 1]
        inner = own[row + 1 : row + 2] + far[t, 2 * p + 1 : 2 * p + 2]
        inverse = 1.0 / total
        return inverse, inner * inverse

    for t in range(tiles):
        load_queries(q_ref, g_ref, t, own_q, own_g, q_unit, q_scale)
        for p in range(pairs):
            total, inner = forward(p, t, 0, t + 1, own_kinds(t), own_q, own_g, own_e, own_p)
            row = stat_row(p, t)
            own_stat[row : row + 1] = total
            own_stat[row + 1 : row + 2] = inner

    @pl.when(has_prev)
    def _():
        own_copy().start()
        for c in in_order[ahead:]:
            c.start()

    @pl.when(jnp.logical_not(has_prev))
    def _():
        stat_recv[...] = jnp.zeros_like(stat_recv)
        dq_recv[...] = jnp.zeros_like(dq_recv)

    meet(0)

    def far_forward(t):
        @pl.when(has_next)
        def _():
            for c in in_copies(t):
                c.wait_recv()
            load_queries(next_q, next_g, t, far_q, far_g, next_unit, None)
            for p in range(pairs):
                total, inner = forward(
                    p, t, t, tiles, far_forward_kinds(t), far_q, far_g, far_e, far_p
                )
                stat_send[t, 2 * p : 2 * p + 1] = total
                stat_send[t, 2 * p + 1 : 2 * p + 2] = inner
            stat_copy(t).start()

    def far_backward(t):
        @pl.when(has_next)
        def _():
            if t == 0:
                own_copy().wait_recv()
            for p in range(pairs):
                inverse, delta = normalizers(p, t, next_stat, stat_send)
                part = backward(
                    p, t, t, tiles, far_forward_kinds(t), far_q, far_g, far_e, far_p, inverse, delta
                )
                dq_send[t, :, pair_lanes(p)] = part.astype(jnp.bfloat16)
                gain_part[...] += jnp.sum(part * next_unit[p, span(t)], axis=0, keepdims=True)

    def dq_start(ts):
        @pl.when(has_next)
        def _():
            for t in ts:
                dq_copy(t).start()

    def own_backward(t):
        @pl.when(has_prev)
        def _():
            stat_copy(t).wait_recv()

        for p in range(pairs):
            inverse, delta = normalizers(p, t, own_stat, stat_recv)
            part = backward(
                p, t, 0, t + 1, own_kinds(t), own_q, own_g, own_e, own_p, inverse, delta
            )
            dq_own[p, span(t)] = part
            gain_part[...] += jnp.sum(part * q_unit[p, span(t)], axis=0, keepdims=True)

    for t in range(tiles):
        far_forward(t)
        if t < tiles - 1:
            far_backward(t)
        if t == min(1, tiles - 1):
            meet(1)
    dq_start(range(tiles - 1))
    far_backward(tiles - 1)
    dq_start(range(tiles - 1, tiles))
    for r in range(2, rounds):
        meet(r)
    for t in range(tiles):
        own_backward(t)

    k_part = jnp.zeros((1, LANES), jnp.float32)
    for p in range(pairs):
        k_part = k_part + jnp.sum(dk[p] * k_unit[p], axis=0, keepdims=True)

    halves = [x + pltpu.roll(x, LANES // 2, 1) for x in (gain_part[...], k_part)]
    first_half = iota((1, LANES), 1) < LANES // 2
    gain_message[...] = jnp.where(first_half, halves[0], halves[1]) * score_scale

    def gain_copy(k, slot, target):
        return pltpu.make_async_remote_copy(
            src_ref=gain_message,
            dst_ref=gain_gathered.at[slot],
            send_sem=gain_send_sem.at[k],
            recv_sem=gain_recv_sem.at[slot],
            device_id={"sp": target // n_tp, "tp": lax.rem(target, n_tp)},
            device_id_type=MESH,
        )

    loop(everyone, lambda k: gain_copy(k, me_flat, flat_peer(k)).start())
    gain_gathered[me_flat] = gain_message[...]

    if message.shape[0] > 2 * heads:
        message[...] = jnp.zeros_like(message)
    for h in range(heads):
        lanes = slice((h % 2) * TILE, (h % 2 + 1) * TILE)
        row = jnp.sum(skew(taps[h // 2, :, lanes], True), axis=0, keepdims=True)
        rest = jnp.sum(totals[h // 2 : h // 2 + 1, lanes], axis=1, keepdims=True) - jnp.sum(
            row, axis=1, keepdims=True
        )
        message[h : h + 1] = row
        message[heads + h : heads + h + 1] = jnp.broadcast_to(rest, (1, LANES))

    def sum_copy(k, slot, target):
        return copy(message, gathered.at[slot], sum_send_sem.at[k], sum_recv_sem.at[slot], target)

    loop(n_sp, lambda k: sum_copy(k, me, sp_peer(k)).start())
    gathered[me] = message[...]

    def norm_backward(unit, scale, grad_hat, gain):
        grad_unit = grad_hat * gain
        inner = half_mean(grad_unit * unit)
        return (scale * (grad_unit - unit * inner)).astype(jnp.bfloat16)

    for p in range(pairs):
        for t in range(tiles):
            here = (p, span(t))
            k_out[span(t), pair_lanes(p)] = norm_backward(
                k_unit[here], k_scale[here], dk[here] * score_scale, k_gain
            )
            v_out[span(t), pair_lanes(p)] = dv[here].astype(jnp.bfloat16)


    for t in range(tiles):

        @pl.when(has_prev)
        def _():
            dq_copy(t).wait_recv()

        for p in range(pairs):
            here = (p, span(t))
            grad_hat = (dq_own[here] + dq_recv[t, :, pair_lanes(p)].astype(jnp.float32)) * score_scale
            q_out[span(t), pair_lanes(p)] = norm_backward(
                q_unit[here], q_scale[here], grad_hat, q_gain
            )

    loop(n_sp, lambda k: sum_copy(k, sp_peer(k), sp_peer(k)).wait_recv())
    summed = jnp.sum(gathered[...], axis=0)
    for h in range(heads):
        bias_out[h : h + 1, 0:CLIP] = summed[h : h + 1]
        bias_out[h : h + 1, CLIP : CLIP + 1] = summed[heads + h : heads + h + 1, 0:1]
    loop(everyone, lambda k: gain_copy(k, flat_peer(k), flat_peer(k)).wait_recv())
    gains = jnp.sum(gain_gathered[...], axis=0)
    q_gain_out[...] = gains[:, 0 : LANES // 2]
    k_gain_out[...] = gains[:, LANES // 2 :]

    loop(n_sp, lambda k: sum_copy(k, me, sp_peer(k)).wait_send())
    loop(everyone, lambda k: gain_copy(k, me_flat, flat_peer(k)).wait_send())

    @pl.when(has_prev)
    def _():
        own_copy().wait_send()
        for c in in_order:
            c.wait_send()

    @pl.when(has_next)
    def _():
        for t in range(tiles):
            stat_copy(t).wait_send()
            dq_copy(t).wait_send()


def place(*refs):
    half = len(refs) // 2
    sem = refs[-1]
    moves = [
        pltpu.make_async_copy(source, target, sem.at[i])
        for i, (source, target) in enumerate(zip(refs[:half], refs[half:-1]))
    ]
    for c in moves:
        c.start()
    for c in moves:
        c.wait()


def per_device(axis_sizes, query, key, value, out_grad, query_gain, key_gain, rel_bias):
    n_sp, n_tp = axis_sizes
    rows, width = query.shape
    heads, taps = rel_bias.shape
    head_width = width // heads
    tiles = rows // TILE
    pairs = width // LANES
    low, full = jnp.bfloat16, jnp.float32
    message_rows = -(-2 * heads // 8) * 8
    stat_rows = -(-2 * pairs // 8) * 8
    vmem = pl.BlockSpec(memory_space=pltpu.VMEM)
    anywhere = pl.BlockSpec(memory_space=pl.ANY)
    stat = pltpu.VMEM((tiles, stat_rows, WIDE), full)
    sums = pltpu.VMEM((-(-2 * pairs * tiles // 8) * 8, WIDE), full)
    wide = pltpu.VMEM((pairs, tiles, WIDE, LANES), low)
    square = pltpu.VMEM((pairs, tiles, rows, WIDE), full)
    units = pltpu.VMEM((pairs, rows, LANES), full)
    dma = pltpu.SemaphoreType.DMA
    results = (
        ((rows, width), low),
        ((rows, width), low),
        ((rows, width), low),
        ((1, head_width), full),
        ((1, head_width), full),
        ((heads, taps), full),
    )
    given = (query, key, value, out_grad, query_gain.reshape(1, -1), key_gain.reshape(1, -1), rel_bias)
    kept = pl.pallas_call(
        functools.partial(kernel, axis_sizes, head_width),
        out_shape=tuple(pltpu.VMEM(shape, kind) for shape, kind in results),
        in_specs=[anywhere] * 7,
        out_specs=(vmem,) * 6,
        scratch_shapes=[pltpu.VMEM((rows, width), low)] * 4
        + [
            pltpu.VMEM((1, head_width), full),
            pltpu.VMEM((1, head_width), full),
            pltpu.VMEM((heads, taps), full),
        ]
        + [
            pltpu.VMEM((rows, width), low),
            pltpu.VMEM((rows, width), low),
            stat,
            stat,
            sums,
            pltpu.VMEM((tiles, TILE, width), low),
            pltpu.VMEM((tiles, TILE, width), low),
            pltpu.VMEM((pairs, rows, LANES), low),
            pltpu.VMEM((pairs, LANES, rows), low),
            wide,
            wide,
            wide,
            wide,
            square,
            square,
            square,
            square,
            pltpu.VMEM((pairs, rows, LANES), full),
            pltpu.VMEM((pairs, rows, LANES), full),
            pltpu.VMEM((pairs, rows, LANES), full),
            pltpu.VMEM((pairs, TILE, WIDE), full),
            pltpu.VMEM((pairs, TILE, WIDE), full),
            pltpu.VMEM((8, WIDE), full),
            sums,
            units,
            units,
            units,
            units,
            units,
            pltpu.VMEM((1, LANES), full),
            pltpu.VMEM((message_rows, LANES), full),
            pltpu.VMEM((n_sp, message_rows, LANES), full),
            pltpu.VMEM((1, LANES), full),
            pltpu.VMEM((n_sp * n_tp, 1, LANES), full),
            dma((2 * tiles,)),
            dma((2 * tiles,)),
            dma((tiles,)),
            dma((tiles,)),
            dma((1,)),
            dma((1,)),
            dma((tiles,)),
            dma((tiles,)),
            dma((n_sp,)),
            dma((n_sp,)),
            dma((n_sp * n_tp,)),
            dma((n_sp * n_tp,)),
            dma((7,)),
            pltpu.SemaphoreType.REGULAR((max((n_sp - 1).bit_length(), 1),)),
        ],
        compiler_params=pltpu.CompilerParams(
            has_side_effects=True, collective_id=0, vmem_limit_bytes=MAIN_VMEM
        ),
    )(*(pltpu.with_memory_space_constraint(x, pltpu.HBM) for x in given))
    query_grad, key_grad, value_grad, query_gain_grad, key_gain_grad, bias_grad = pl.pallas_call(
        place,
        out_shape=tuple(jax.ShapeDtypeStruct(shape, kind) for shape, kind in results),
        in_specs=[vmem] * 6,
        out_specs=(anywhere,) * 6,
        scratch_shapes=[dma((6,))],
        compiler_params=pltpu.CompilerParams(vmem_limit_bytes=PLACE_VMEM),
    )(*kept)
    return (
        query_grad,
        key_grad,
        value_grad,
        query_gain_grad.reshape(-1),
        key_gain_grad.reshape(-1),
        bias_grad,
    )


def solution(mesh):
    axis_sizes = (mesh.shape["sp"], mesh.shape["tp"])
    placed = (P("sp", "tp"), P("sp", "tp"), P("sp", "tp"), P("sp", "tp"), P(), P(), P("tp", None))
    return jax.shard_map(
        functools.partial(per_device, axis_sizes),
        mesh=mesh,
        in_specs=placed,
        out_specs=(P("sp", "tp"), P("sp", "tp"), P("sp", "tp"), P(), P(), P("tp", None)),
        check_vma=False,
    )
```

```python
import functools

import jax
import jax.numpy as jnp
from jax import lax
from jax.experimental import pallas as pl
from jax.experimental.pallas import tpu as pltpu
from jax.sharding import PartitionSpec as P

CLIP = 128
TILE = 128
LANES = 128
WIDE = 2 * TILE
EPSILON = 1e-06
LOG2E = 1.4426950408889634
MASKED = -1e30
MAIN_VMEM = 48 * 1024 * 1024
PLACE_VMEM = 4 * 1024 * 1024
MESH = pl.DeviceIdType.MESH
NT = (((1,), (1,)), ((), ()))
NN = (((1,), (0,)), ((), ()))


def dot(a, b, dims=NN):
    return lax.dot_general(a, b, dims, preferred_element_type=jnp.float32)


def iota(shape, axis):
    return lax.broadcasted_iota(jnp.int32, shape, axis)


def half_mean(x):
    low = iota(x.shape, 1) < LANES // 2
    first = jnp.sum(jnp.where(low, x, 0.0), axis=1, keepdims=True)
    second = jnp.sum(jnp.where(low, 0.0, x), axis=1, keepdims=True)
    return jnp.where(low, first, second) * (2.0 / LANES)


def unit_of(x):
    scale = lax.rsqrt(half_mean(x * x) + EPSILON)
    return x * scale, scale


def low_skew(x, left):
    row = iota(x.shape, 0)
    for bit in range(3):
        step = 1 << bit
        moved = pltpu.roll(x, LANES - step if left else step, 1)
        x = jnp.where((row & step) != 0, moved, x)
    return x


def by_distance(table):
    first = low_skew(jnp.broadcast_to(table, (8, LANES)), False)
    blocks = [first] + [pltpu.roll(first, at, 1) for at in range(8, TILE, 8)]
    return jnp.concatenate(blocks, axis=0)


def distance_sums(x):
    total = x[0:8]
    for at in range(8, TILE, 8):
        total = total + pltpu.roll(x[at : at + 8], LANES - at, 1)
    return jnp.sum(low_skew(total, True), axis=0, keepdims=True)


def kernel(
    axis_sizes,
    head_width,
    q_hbm,
    k_hbm,
    v_hbm,
    g_hbm,
    q_gain_hbm,
    k_gain_hbm,
    bias_hbm,
    q_out,
    k_out,
    v_out,
    q_gain_out,
    k_gain_out,
    bias_out,
    q_ref,
    k_ref,
    v_ref,
    g_ref,
    q_gain_ref,
    k_gain_ref,
    bias_ref,
    next_q,
    next_g,
    prev_k,
    prev_v,
    prev_hat,
    prev_turned,
    prev_unit,
    side_send,
    side_recv,
    k_gain_part,
    stat_send,
    stat_recv,
    next_stat,
    dq_send,
    dq_recv,
    k_hat,
    k_turned,
    own_q,
    own_g,
    far_q,
    far_g,
    own_e,
    own_p,
    far_e,
    far_p,
    dk,
    dv,
    dq_own,
    near_bias,
    taps,
    totals,
    own_stat,
    q_unit,
    q_scale,
    next_unit,
    k_unit,
    k_scale,
    gain_part,
    message,
    gathered,
    gain_message,
    gain_gathered,
    in_send_sem,
    in_recv_sem,
    stat_send_sem,
    stat_recv_sem,
    own_send_sem,
    own_recv_sem,
    dq_send_sem,
    dq_recv_sem,
    sum_send_sem,
    sum_recv_sem,
    gain_send_sem,
    gain_recv_sem,
    load_sem,
    met_sem,
    kv_send_sem,
    kv_recv_sem,
    side_send_sem,
    side_recv_sem,
):
    n_sp, n_tp = axis_sizes
    rows, width = q_hbm.shape
    tiles = rows // TILE
    last = tiles - 1
    pairs = width // LANES
    heads = 2 * pairs
    score_scale = head_width ** (-0.5)
    me = lax.axis_index("sp")
    me_tp = lax.axis_index("tp")
    has_prev = me > 0
    has_next = me < n_sp - 1
    before = jnp.maximum(me - 1, 0)
    after = jnp.minimum(me + 1, n_sp - 1)

    def span(t):
        return slice(t * TILE, (t + 1) * TILE)

    def pair_lanes(p):
        return slice(p * LANES, (p + 1) * LANES)

    def copy(src, dst, send, recv, target):
        return pltpu.make_async_remote_copy(
            src_ref=src,
            dst_ref=dst,
            send_sem=send,
            recv_sem=recv,
            device_id={"sp": target},
            device_id_type=MESH,
        )

    def in_copies(t):
        return (
            copy(q_ref.at[span(t)], next_q.at[span(t)], in_send_sem.at[2 * t], in_recv_sem.at[2 * t], before),
            copy(g_ref.at[span(t)], next_g.at[span(t)], in_send_sem.at[2 * t + 1], in_recv_sem.at[2 * t + 1], before),
        )

    def stat_copy(t):
        return copy(stat_send.at[t], stat_recv.at[t], stat_send_sem.at[t], stat_recv_sem.at[t], after)

    def own_copy():
        return copy(own_stat, next_stat, own_send_sem.at[0], own_recv_sem.at[0], before)

    def dq_copy(t):
        return copy(dq_send.at[t], dq_recv.at[t], dq_send_sem.at[t], dq_recv_sem.at[t], after)

    def kv_copies():
        return (
            copy(k_ref.at[span(last)], prev_k, kv_send_sem.at[0], kv_recv_sem.at[0], after),
            copy(v_ref.at[span(last)], prev_v, kv_send_sem.at[1], kv_recv_sem.at[1], after),
        )

    def side_copy():
        return copy(side_send, side_recv, side_send_sem.at[0], side_recv_sem.at[0], before)

    def loop(count, body):
        def step(i, carry):
            body(i + 1)
            return carry

        lax.fori_loop(0, count - 1, step, 0)

    def sp_peer(k):
        return lax.rem(me + k, n_sp)

    def tp_peer(k):
        return lax.rem(me_tp + k, n_tp)

    everyone = n_sp * n_tp
    me_flat = me * n_tp + me_tp

    def flat_peer(k):
        return lax.rem(me_flat + k, everyone)

    barrier = pltpu.get_barrier_semaphore()

    def greet(target):
        pl.semaphore_signal(barrier, inc=1, device_id=target, device_id_type=MESH)

    pl.when(has_prev)(lambda: greet({"sp": before}))
    pl.when(has_next)(lambda: greet({"sp": after}))
    loop(n_tp, lambda k: greet({"tp": tp_peer(k)}))
    moves = (
        (q_hbm, q_ref),
        (g_hbm, g_ref),
        (k_hbm, k_ref),
        (v_hbm, v_ref),
        (q_gain_hbm, q_gain_ref),
        (k_gain_hbm, k_gain_ref),
        (bias_hbm, bias_ref),
    )
    loads = [pltpu.make_async_copy(a, b, load_sem.at[i]) for i, (a, b) in enumerate(moves)]
    for c in loads:
        c.start()
    pl.semaphore_wait(barrier, has_prev.astype(jnp.int32) + has_next.astype(jnp.int32) + n_tp - 1)
    rounds = met_sem.shape[0]

    def round_signal(r):
        for ok, target in ((me >= 1 << r, me - (1 << r)), (me + (1 << r) < n_sp, me + (1 << r))):

            @pl.when(ok)
            def _():
                pl.semaphore_signal(
                    met_sem.at[r], inc=1, device_id={"sp": target}, device_id_type=MESH
                )

    def round_wait(r):
        count = (me >= 1 << r).astype(jnp.int32) + (me + (1 << r) < n_sp).astype(jnp.int32)
        pl.semaphore_wait(met_sem.at[r], count)

    def meet(r):
        if r < rounds:
            round_wait(r)
        if r + 1 < rounds:
            round_signal(r + 1)

    round_signal(0)
    loads[0].wait()
    loads[1].wait()

    in_order = [c for t in range(last) for c in in_copies(t)]
    ahead = min(3, len(in_order))

    @pl.when(has_prev)
    def _():
        for c in in_order[:ahead]:
            c.start()

    for c in loads[2:]:
        c.wait()
    q_gain = jnp.concatenate([q_gain_ref[...]] * 2, axis=1)
    k_gain = jnp.concatenate([k_gain_ref[...]] * 2, axis=1)
    low_lane = iota((TILE, LANES), 1) < LANES // 2

    def split_heads(x):
        first = jnp.where(low_lane, x, 0.0)
        second = jnp.where(low_lane, 0.0, x)
        return jnp.concatenate([first, second], axis=0).astype(jnp.bfloat16)

    def load_queries(q_from, g_from, t, q_to, g_to, unit_to, scale_to):
        for p in range(pairs):
            x = q_from[span(t), pair_lanes(p)].astype(jnp.float32)
            unit, scale = unit_of(x)
            unit_to[p, span(t)] = unit
            if scale_to is not None:
                scale_to[p, span(t)] = scale
            q_to[p, t] = split_heads(unit * q_gain)
            g_to[p, t] = split_heads(g_from[span(t), pair_lanes(p)].astype(jnp.float32))

    key_at = iota((TILE, WIDE), 0)
    query_at = iota((TILE, WIDE), 1) % TILE
    causal = query_at >= key_at
    far_bias = jnp.where((key_at // 64) >= (query_at // 64), 0.0, MASKED)

    edge_bias = far_bias + jnp.where(has_prev, 0.0, MASKED)

    for p in range(pairs):
        for t in range(tiles):
            x = k_ref[span(t), pair_lanes(p)].astype(jnp.float32)
            unit, scale = unit_of(x)
            k_unit[p, span(t)] = unit
            k_scale[p, span(t)] = scale
            hat = unit * k_gain
            k_hat[p, span(t)] = hat.astype(jnp.bfloat16)
            k_turned[p, :, span(t)] = hat.T.astype(jnp.bfloat16)
        sheets = []
        for h in (2 * p, 2 * p + 1):
            table = (bias_ref[h : h + 1, 0:CLIP] - bias_ref[h : h + 1, CLIP : CLIP + 1]) * LOG2E
            sheets.append(by_distance(table))
        near_bias[p] = jnp.concatenate(sheets, axis=1)
    dk[...] = jnp.zeros_like(dk)
    dv[...] = jnp.zeros_like(dv)
    taps[...] = jnp.zeros_like(taps)
    totals[...] = jnp.zeros_like(totals)
    gain_part[...] = jnp.zeros_like(gain_part)
    k_gain_part[...] = jnp.zeros_like(k_gain_part)

    def forward(p, t, start, stop, kinds, q_from, g_from, e_to, p_to):
        keys = slice(start * TILE, stop * TILE)
        raw = dot(k_hat[p, keys], q_from[p, t], NT)
        grad = dot(v_ref[keys, pair_lanes(p)], g_from[p, t], NT)
        total = jnp.zeros((1, WIDE), jnp.float32)
        inner = jnp.zeros((1, WIDE), jnp.float32)
        for c in range(start, stop):
            here = slice((c - start) * TILE, (c - start + 1) * TILE)
            s = raw[here] * (score_scale * LOG2E)
            kind = kinds.get(c)
            if kind == "diagonal":
                s = jnp.where(causal, s + near_bias[p], MASKED)
            elif kind == "below":
                s = s + jnp.where(causal, 0.0, near_bias[p])
            elif kind == "far":
                s = s + far_bias
            e = jnp.exp2(s)
            dp = grad[here]
            e_to[p, t, span(c)] = e
            p_to[p, t, span(c)] = dp
            total = total + jnp.sum(e, axis=0, keepdims=True)
            inner = inner + jnp.sum(e * dp, axis=0, keepdims=True)
        return total, inner

    def backward(p, t, start, stop, kinds, q_from, g_from, e_from, p_from, inverse, delta):
        keys = slice(start * TILE, stop * TILE)
        attention = e_from[p, t, keys] * inverse
        grad = attention * (p_from[p, t, keys] - delta)
        attention_low = attention.astype(jnp.bfloat16)
        grad_low = grad.astype(jnp.bfloat16)
        dv[p, keys] += dot(attention_low, g_from[p, t])
        dk[p, keys] += dot(grad_low, q_from[p, t])
        turned = dot(k_turned[p, :, keys], grad_low)
        totals[p : p + 1] += jnp.sum(grad, axis=0, keepdims=True)
        for c, kind in kinds.items():
            part = grad[(c - start) * TILE : (c - start + 1) * TILE]
            if kind == "diagonal":
                taps[p] += part
            elif kind == "below":
                taps[p] += jnp.where(causal, 0.0, part)
        return turned_back(turned)

    def turned_back(turned):
        upper = iota((LANES, TILE), 0) < LANES // 2
        return jnp.where(upper, turned[:, :TILE], turned[:, TILE:]).T

    def own_kinds(t):
        kinds = {t: "diagonal"}
        if t > 0:
            kinds[t - 1] = "below"
        return kinds

    def far_forward_kinds(t):
        kinds = {t: "far"}
        if t == 0:
            kinds[tiles - 1] = "below"
        return kinds

    def stat_row(p, t):
        return 2 * (t * pairs + p)

    def normalizers(p, t, own, far):
        row = stat_row(p, t)
        total = own[row : row + 1] + far[t, 2 * p : 2 * p + 1]
        inner = own[row + 1 : row + 2] + far[t, 2 * p + 1 : 2 * p + 2]
        inverse = 1.0 / total
        return inverse, inner * inverse

    for t in range(tiles):
        load_queries(q_ref, g_ref, t, own_q, own_g, q_unit, q_scale)
        for p in range(pairs):
            total, inner = forward(p, t, 0, t + 1, own_kinds(t), own_q, own_g, own_e, own_p)
            row = stat_row(p, t)
            own_stat[row : row + 1] = total
            own_stat[row + 1 : row + 2] = inner

    @pl.when(has_prev)
    def _():
        own_copy().start()
        for c in in_order[ahead:]:
            c.start()

    @pl.when(jnp.logical_not(has_prev))
    def _():
        stat_recv[...] = jnp.zeros_like(stat_recv)
        prev_k[...] = jnp.zeros_like(prev_k)
        prev_v[...] = jnp.zeros_like(prev_v)
        dq_recv[...] = jnp.zeros_like(dq_recv)

    @pl.when(jnp.logical_not(has_next))
    def _():
        side_recv[...] = jnp.zeros_like(side_recv)

    meet(0)

    def far_forward(t):
        @pl.when(has_next)
        def _():
            for c in in_copies(t):
                c.wait_recv()
            load_queries(next_q, next_g, t, far_q, far_g, next_unit, None)
            for p in range(pairs):
                total, inner = forward(
                    p, t, t, tiles, far_forward_kinds(t), far_q, far_g, far_e, far_p
                )
                stat_send[t, 2 * p : 2 * p + 1] = total
                stat_send[t, 2 * p + 1 : 2 * p + 2] = inner
            stat_copy(t).start()

    def far_backward(t):
        @pl.when(has_next)
        def _():
            if t == 0:
                own_copy().wait_recv()
            for p in range(pairs):
                inverse, delta = normalizers(p, t, next_stat, stat_send)
                part = backward(
                    p, t, t, tiles, far_forward_kinds(t), far_q, far_g, far_e, far_p, inverse, delta
                )
                dq_send[t, :, pair_lanes(p)] = part.astype(jnp.bfloat16)
                gain_part[...] += jnp.sum(part * next_unit[p, span(t)], axis=0, keepdims=True)

    def dq_start(ts):
        @pl.when(has_next)
        def _():
            for t in ts:
                dq_copy(t).start()

    def side_forward(t):
        @pl.when(has_prev)
        def _():
            for c in kv_copies():
                c.wait_recv()

        for p in range(pairs):
            unit, _ = unit_of(prev_k[:, pair_lanes(p)].astype(jnp.float32))
            prev_unit[p] = unit
            hat = unit * k_gain
            prev_hat[p] = hat.astype(jnp.bfloat16)
            prev_turned[p] = hat.T.astype(jnp.bfloat16)
            raw = dot(prev_hat[p], own_q[p, t], NT)
            dp = dot(prev_v[:, pair_lanes(p)], own_g[p, t], NT)
            e = jnp.exp2(raw * (score_scale * LOG2E) + edge_bias)
            far_e[p, t, span(t)] = e
            far_p[p, t, span(t)] = dp
            stat_recv[t, 2 * p : 2 * p + 1] = jnp.sum(e, axis=0, keepdims=True)
            stat_recv[t, 2 * p + 1 : 2 * p + 2] = jnp.sum(e * dp, axis=0, keepdims=True)

    def side_backward(t):
        for p in range(pairs):
            inverse, delta = normalizers(p, t, own_stat, stat_recv)
            attention = far_e[p, t, span(t)] * inverse
            grad = attention * (far_p[p, t, span(t)] - delta)
            attention_low = attention.astype(jnp.bfloat16)
            grad_low = grad.astype(jnp.bfloat16)
            dk_part = dot(grad_low, own_q[p, t])
            side_send[0, :, pair_lanes(p)] = dk_part.astype(jnp.bfloat16)
            side_send[1, :, pair_lanes(p)] = dot(attention_low, own_g[p, t]).astype(jnp.bfloat16)
            k_gain_part[...] += jnp.sum(dk_part * prev_unit[p], axis=0, keepdims=True)
            totals[p : p + 1] += jnp.sum(grad, axis=0, keepdims=True)
            part = turned_back(dot(prev_turned[p], grad_low))
            dq_own[p, span(t)] += part
            gain_part[...] += jnp.sum(part * q_unit[p, span(t)], axis=0, keepdims=True)

    def kv_start():
        @pl.when(has_next)
        def _():
            for c in kv_copies():
                c.start()

    def side_start():
        pl.when(has_prev)(lambda: side_copy().start())

    def own_backward(t):
        if t < last:

            @pl.when(has_prev)
            def _():
                stat_copy(t).wait_recv()

        for p in range(pairs):
            inverse, delta = normalizers(p, t, own_stat, stat_recv)
            part = backward(
                p, t, 0, t + 1, own_kinds(t), own_q, own_g, own_e, own_p, inverse, delta
            )
            dq_own[p, span(t)] = part
            gain_part[...] += jnp.sum(part * q_unit[p, span(t)], axis=0, keepdims=True)

    for t in range(last):
        far_forward(t)
        far_backward(t)
        if t == max(last - 2, 0):
            kv_start()
        if t == min(1, last):
            meet(1)
    for r in range(2, rounds):
        meet(r)
    early = max(last - 1, 0)
    dq_start(range(early))
    for t in range(last - 1):
        own_backward(t)
    side_forward(last)
    own_backward(last)
    side_backward(last)
    own_backward(last - 1)

    k_part = k_gain_part[...]
    for p in range(pairs):
        k_part = k_part + jnp.sum(dk[p] * k_unit[p], axis=0, keepdims=True)

    halves = [x + pltpu.roll(x, LANES // 2, 1) for x in (gain_part[...], k_part)]
    first_half = iota((1, LANES), 1) < LANES // 2
    gain_message[...] = jnp.where(first_half, halves[0], halves[1]) * score_scale

    def gain_copy(slot, target):
        return pltpu.make_async_remote_copy(
            src_ref=gain_message,
            dst_ref=gain_gathered.at[slot],
            send_sem=gain_send_sem.at[0],
            recv_sem=gain_recv_sem.at[0],
            device_id={"sp": target // n_tp, "tp": lax.rem(target, n_tp)},
            device_id_type=MESH,
        )

    loop(everyone, lambda k: gain_copy(me_flat, flat_peer(k)).start())
    gain_gathered[me_flat] = gain_message[...]

    if message.shape[0] > 2 * heads:
        message[...] = jnp.zeros_like(message)
    for h in range(heads):
        lanes = slice((h % 2) * TILE, (h % 2 + 1) * TILE)
        row = distance_sums(taps[h // 2, :, lanes])
        rest = jnp.sum(totals[h // 2 : h // 2 + 1, lanes], axis=1, keepdims=True) - jnp.sum(
            row, axis=1, keepdims=True
        )
        message[h : h + 1] = row
        message[heads + h : heads + h + 1] = jnp.broadcast_to(rest, (1, LANES))

    def sum_copy(slot, target):
        return copy(message, gathered.at[slot], sum_send_sem.at[0], sum_recv_sem.at[0], target)

    loop(n_sp, lambda k: sum_copy(me, sp_peer(k)).start())
    gathered[me] = message[...]
    dq_start(range(early, last))
    side_start()

    def norm_backward(unit, scale, grad_hat, gain):
        grad_unit = grad_hat * gain
        inner = half_mean(grad_unit * unit)
        return (scale * (grad_unit - unit * inner)).astype(jnp.bfloat16)

    def finish_keys(t, dk_more, dv_more):
        for p in range(pairs):
            here = (p, span(t))
            dk_all, dv_all = dk[here], dv[here]
            if dk_more is not None:
                dk_all = dk_all + dk_more[:, pair_lanes(p)].astype(jnp.float32)
                dv_all = dv_all + dv_more[:, pair_lanes(p)].astype(jnp.float32)
            k_out[span(t), pair_lanes(p)] = norm_backward(
                k_unit[here], k_scale[here], dk_all * score_scale, k_gain
            )
            v_out[span(t), pair_lanes(p)] = dv_all.astype(jnp.bfloat16)

    def finish_queries(t, dq_more):
        for p in range(pairs):
            here = (p, span(t))
            dq_all = dq_own[here]
            if dq_more is not None:
                dq_all = dq_all + dq_more[:, pair_lanes(p)].astype(jnp.float32)
            q_out[span(t), pair_lanes(p)] = norm_backward(
                q_unit[here], q_scale[here], dq_all * score_scale, q_gain
            )

    for t in range(last):
        finish_keys(t, None, None)
    finish_queries(last, None)
    for t in range(last):

        @pl.when(has_prev)
        def _():
            dq_copy(t).wait_recv()

        finish_queries(t, dq_recv.at[t])

    @pl.when(has_next)
    def _():
        side_copy().wait_recv()

    finish_keys(last, side_recv.at[0], side_recv.at[1])
    def drain():
        @pl.when(has_prev)
        def _():
            own_copy().wait_send()
            side_copy().wait_send()
            for c in in_order:
                c.wait_send()

        @pl.when(has_next)
        def _():
            for c in kv_copies():
                c.wait_send()
            for t in range(last):
                stat_copy(t).wait_send()
                dq_copy(t).wait_send()

    all_sums = gathered.at[0 : n_sp - 1]
    all_sums = copy(all_sums, all_sums, sum_send_sem.at[0], sum_recv_sem.at[0], before)
    all_gains = gain_gathered.at[0 : everyone - 1]
    all_gains = copy(all_gains, all_gains, gain_send_sem.at[0], gain_recv_sem.at[0], before)
    all_sums.wait_send()
    all_gains.wait_send()
    drain()
    all_sums.wait_recv()
    summed = jnp.sum(gathered[...], axis=0)
    for h in range(heads):
        bias_out[h : h + 1, 0:CLIP] = summed[h : h + 1]
        bias_out[h : h + 1, CLIP : CLIP + 1] = summed[heads + h : heads + h + 1, 0:1]
    all_gains.wait_recv()
    gains = jnp.sum(gain_gathered[...], axis=0)
    q_gain_out[...] = gains[:, 0 : LANES // 2]
    k_gain_out[...] = gains[:, LANES // 2 :]


def place(*refs):
    half = len(refs) // 2
    sem = refs[-1]
    moves = [
        pltpu.make_async_copy(source, target, sem.at[i])
        for i, (source, target) in enumerate(zip(refs[:half], refs[half:-1]))
    ]
    for c in moves:
        c.start()
    for c in moves:
        c.wait()


def per_device(axis_sizes, query, key, value, out_grad, query_gain, key_gain, rel_bias):
    n_sp, n_tp = axis_sizes
    rows, width = query.shape
    heads, taps = rel_bias.shape
    head_width = width // heads
    tiles = rows // TILE
    pairs = width // LANES
    low, full = jnp.bfloat16, jnp.float32
    message_rows = -(-2 * heads // 8) * 8
    stat_rows = -(-2 * pairs // 8) * 8
    vmem = pl.BlockSpec(memory_space=pltpu.VMEM)
    anywhere = pl.BlockSpec(memory_space=pl.ANY)
    stat = pltpu.VMEM((tiles, stat_rows, WIDE), full)
    sums = pltpu.VMEM((-(-2 * pairs * tiles // 8) * 8, WIDE), full)
    wide = pltpu.VMEM((pairs, tiles, WIDE, LANES), low)
    square = pltpu.VMEM((pairs, tiles, rows, WIDE), full)
    units = pltpu.VMEM((pairs, rows, LANES), full)
    dma = pltpu.SemaphoreType.DMA
    results = (
        ((rows, width), low),
        ((rows, width), low),
        ((rows, width), low),
        ((1, head_width), full),
        ((1, head_width), full),
        ((heads, taps), full),
    )
    given = (query, key, value, out_grad, query_gain.reshape(1, -1), key_gain.reshape(1, -1), rel_bias)
    kept = pl.pallas_call(
        functools.partial(kernel, axis_sizes, head_width),
        out_shape=tuple(pltpu.VMEM(shape, kind) for shape, kind in results),
        in_specs=[anywhere] * 7,
        out_specs=(vmem,) * 6,
        scratch_shapes=[pltpu.VMEM((rows, width), low)] * 4
        + [
            pltpu.VMEM((1, head_width), full),
            pltpu.VMEM((1, head_width), full),
            pltpu.VMEM((heads, taps), full),
        ]
        + [
            pltpu.VMEM((rows, width), low),
            pltpu.VMEM((rows, width), low),
            pltpu.VMEM((TILE, width), low),
            pltpu.VMEM((TILE, width), low),
            pltpu.VMEM((pairs, TILE, LANES), low),
            pltpu.VMEM((pairs, LANES, TILE), low),
            pltpu.VMEM((pairs, TILE, LANES), full),
            pltpu.VMEM((2, TILE, width), low),
            pltpu.VMEM((2, TILE, width), low),
            pltpu.VMEM((1, LANES), full),
            stat,
            stat,
            sums,
            pltpu.VMEM((tiles, TILE, width), low),
            pltpu.VMEM((tiles, TILE, width), low),
            pltpu.VMEM((pairs, rows, LANES), low),
            pltpu.VMEM((pairs, LANES, rows), low),
            wide,
            wide,
            wide,
            wide,
            square,
            square,
            square,
            square,
            pltpu.VMEM((pairs, rows, LANES), full),
            pltpu.VMEM((pairs, rows, LANES), full),
            pltpu.VMEM((pairs, rows, LANES), full),
            pltpu.VMEM((pairs, TILE, WIDE), full),
            pltpu.VMEM((pairs, TILE, WIDE), full),
            pltpu.VMEM((8, WIDE), full),
            sums,
            units,
            units,
            units,
            units,
            units,
            pltpu.VMEM((1, LANES), full),
            pltpu.VMEM((message_rows, LANES), full),
            pltpu.VMEM((n_sp, message_rows, LANES), full),
            pltpu.VMEM((1, LANES), full),
            pltpu.VMEM((n_sp * n_tp, 1, LANES), full),
            dma((2 * tiles,)),
            dma((2 * tiles,)),
            dma((tiles,)),
            dma((tiles,)),
            dma((1,)),
            dma((1,)),
            dma((tiles,)),
            dma((tiles,)),
            dma((1,)),
            dma((1,)),
            dma((1,)),
            dma((1,)),
            dma((7,)),
            pltpu.SemaphoreType.REGULAR((max((n_sp - 1).bit_length(), 1),)),
            dma((2,)),
            dma((2,)),
            dma((1,)),
            dma((1,)),
        ],
        compiler_params=pltpu.CompilerParams(
            has_side_effects=True, collective_id=0, vmem_limit_bytes=MAIN_VMEM
        ),
    )(*(pltpu.with_memory_space_constraint(x, pltpu.HBM) for x in given))
    query_grad, key_grad, value_grad, query_gain_grad, key_gain_grad, bias_grad = pl.pallas_call(
        place,
        out_shape=tuple(jax.ShapeDtypeStruct(shape, kind) for shape, kind in results),
        in_specs=[vmem] * 6,
        out_specs=(anywhere,) * 6,
        scratch_shapes=[dma((6,))],
        compiler_params=pltpu.CompilerParams(vmem_limit_bytes=PLACE_VMEM),
    )(*kept)
    return (
        query_grad,
        key_grad,
        value_grad,
        query_gain_grad.reshape(-1),
        key_gain_grad.reshape(-1),
        bias_grad,
    )


def solution(mesh):
    axis_sizes = (mesh.shape["sp"], mesh.shape["tp"])
    placed = (P("sp", "tp"), P("sp", "tp"), P("sp", "tp"), P("sp", "tp"), P(), P(), P("tp", None))
    return jax.shard_map(
        functools.partial(per_device, axis_sizes),
        mesh=mesh,
        in_specs=placed,
        out_specs=(P("sp", "tp"), P("sp", "tp"), P("sp", "tp"), P(), P(), P("tp", None)),
        check_vma=False,
    )
```

```python
import functools

import jax
import jax.numpy as jnp
from jax import lax
from jax.experimental import pallas as pl
from jax.experimental.pallas import tpu as pltpu
from jax.sharding import PartitionSpec as P

CLIP = 128
TILE = 128
LANES = 128
WIDE = 2 * TILE
EPSILON = 1e-06
LOG2E = 1.4426950408889634
MASKED = -1e30
MAIN_VMEM = 48 * 1024 * 1024
PLACE_VMEM = 4 * 1024 * 1024
MESH = pl.DeviceIdType.MESH
NT = (((1,), (1,)), ((), ()))
NN = (((1,), (0,)), ((), ()))


def dot(a, b, dims=NN):
    return lax.dot_general(a, b, dims, preferred_element_type=jnp.float32)


def iota(shape, axis):
    return lax.broadcasted_iota(jnp.int32, shape, axis)


def half_mean(x):
    low = iota(x.shape, 1) < LANES // 2
    first = jnp.sum(jnp.where(low, x, 0.0), axis=1, keepdims=True)
    second = jnp.sum(jnp.where(low, 0.0, x), axis=1, keepdims=True)
    return jnp.where(low, first, second) * (2.0 / LANES)


def unit_of(x):
    scale = lax.rsqrt(half_mean(x * x) + EPSILON)
    return x * scale, scale


def low_skew(x, left):
    row = iota(x.shape, 0)
    for bit in range(3):
        step = 1 << bit
        moved = pltpu.roll(x, LANES - step if left else step, 1)
        x = jnp.where((row & step) != 0, moved, x)
    return x


def by_distance(table):
    first = low_skew(jnp.broadcast_to(table, (8, LANES)), False)
    blocks = [first] + [pltpu.roll(first, at, 1) for at in range(8, TILE, 8)]
    return jnp.concatenate(blocks, axis=0)


def distance_sums(x):
    total = x[0:8]
    for at in range(8, TILE, 8):
        total = total + pltpu.roll(x[at : at + 8], LANES - at, 1)
    return jnp.sum(low_skew(total, True), axis=0, keepdims=True)


def kernel(
    axis_sizes,
    head_width,
    q_hbm,
    k_hbm,
    v_hbm,
    g_hbm,
    q_gain_hbm,
    k_gain_hbm,
    bias_hbm,
    q_out,
    k_out,
    v_out,
    q_gain_out,
    k_gain_out,
    bias_out,
    qg_ref,
    kv_ref,
    q_gain_ref,
    k_gain_ref,
    bias_ref,
    next_qg,
    prev_kv,
    prev_hat,
    prev_turned,
    prev_unit,
    side_send,
    side_recv,
    k_gain_part,
    stat_send,
    stat_recv,
    next_stat,
    dq_send,
    dq_recv,
    k_hat,
    k_turned,
    own_q,
    own_g,
    far_q,
    far_g,
    own_e,
    own_p,
    far_e,
    far_p,
    dk,
    dv,
    dq_own,
    near_bias,
    taps,
    totals,
    own_stat,
    q_unit,
    q_scale,
    next_unit,
    k_unit,
    k_scale,
    gain_part,
    message,
    gathered,
    gain_message,
    gain_gathered,
    in_send_sem,
    in_recv_sem,
    stat_send_sem,
    stat_recv_sem,
    own_send_sem,
    own_recv_sem,
    dq_send_sem,
    dq_recv_sem,
    sum_send_sem,
    sum_recv_sem,
    gain_send_sem,
    gain_recv_sem,
    load_sem,
    met_sem,
    kv_send_sem,
    kv_recv_sem,
    side_send_sem,
    side_recv_sem,
):
    n_sp, n_tp = axis_sizes
    rows, width = q_hbm.shape
    tiles = rows // TILE
    last = tiles - 1
    pairs = width // LANES
    heads = 2 * pairs
    score_scale = head_width ** (-0.5)
    me = lax.axis_index("sp")
    me_tp = lax.axis_index("tp")
    has_prev = me > 0
    has_next = me < n_sp - 1
    before = jnp.maximum(me - 1, 0)
    after = jnp.minimum(me + 1, n_sp - 1)

    q_ref, g_ref = qg_ref.at[0], qg_ref.at[1]
    k_ref, v_ref = kv_ref.at[0], kv_ref.at[1]
    next_q, next_g = next_qg.at[0], next_qg.at[1]
    prev_k, prev_v = prev_kv.at[0], prev_kv.at[1]

    def span(t):
        return slice(t * TILE, (t + 1) * TILE)

    def pair_lanes(p):
        return slice(p * LANES, (p + 1) * LANES)

    def copy(src, dst, send, recv, target):
        return pltpu.make_async_remote_copy(
            src_ref=src,
            dst_ref=dst,
            send_sem=send,
            recv_sem=recv,
            device_id={"sp": target},
            device_id_type=MESH,
        )

    def in_copy(t):
        return copy(
            qg_ref.at[:, span(t)], next_qg.at[:, span(t)], in_send_sem.at[t], in_recv_sem.at[t], before
        )

    def stat_copy(t):
        return copy(stat_send.at[t], stat_recv.at[t], stat_send_sem.at[t], stat_recv_sem.at[t], after)

    def own_copy():
        return copy(own_stat, next_stat, own_send_sem.at[0], own_recv_sem.at[0], before)

    def dq_copy(t):
        return copy(dq_send.at[t], dq_recv.at[t], dq_send_sem.at[t], dq_recv_sem.at[t], after)

    def kv_copy():
        return copy(kv_ref.at[:, span(last)], prev_kv, kv_send_sem.at[0], kv_recv_sem.at[0], after)

    def side_copy():
        return copy(side_send, side_recv, side_send_sem.at[0], side_recv_sem.at[0], before)

    def loop(count, body):
        def step(i, carry):
            body(i + 1)
            return carry

        lax.fori_loop(0, count - 1, step, 0)

    def sp_peer(k):
        return lax.rem(me + k, n_sp)

    def tp_peer(k):
        return lax.rem(me_tp + k, n_tp)

    everyone = n_sp * n_tp
    me_flat = me * n_tp + me_tp

    def flat_peer(k):
        return lax.rem(me_flat + k, everyone)

    barrier = pltpu.get_barrier_semaphore()

    def greet(target):
        pl.semaphore_signal(barrier, inc=1, device_id=target, device_id_type=MESH)

    pl.when(has_prev)(lambda: greet({"sp": before}))
    pl.when(has_next)(lambda: greet({"sp": after}))
    pl.when(me == 0)(lambda: loop(n_tp, lambda k: greet({"tp": tp_peer(k)})))
    moves = (
        (q_hbm, q_ref),
        (g_hbm, g_ref),
        (k_hbm, k_ref),
        (v_hbm, v_ref),
        (q_gain_hbm, q_gain_ref),
        (k_gain_hbm, k_gain_ref),
        (bias_hbm, bias_ref),
    )
    loads = [pltpu.make_async_copy(a, b, load_sem.at[i]) for i, (a, b) in enumerate(moves)]
    for c in loads:
        c.start()
    neighbours = has_prev.astype(jnp.int32) + has_next.astype(jnp.int32)
    pl.semaphore_wait(barrier, neighbours + jnp.where(me == 0, n_tp - 1, 0))
    rounds = met_sem.shape[0] - 2

    def round_signal(r):
        for ok, target in ((me >= 1 << r, me - (1 << r)), (me + (1 << r) < n_sp, me + (1 << r))):

            @pl.when(ok)
            def _():
                pl.semaphore_signal(
                    met_sem.at[r], inc=1, device_id={"sp": target}, device_id_type=MESH
                )

    def round_wait(r):
        count = (me >= 1 << r).astype(jnp.int32) + (me + (1 << r) < n_sp).astype(jnp.int32)
        pl.semaphore_wait(met_sem.at[r], count)

    def meet(r):
        if r < rounds:
            round_wait(r)
        if r + 1 < rounds:
            round_signal(r + 1)

    def column_met():
        @pl.when(me == 0)
        def _():
            def tell(k):
                pl.semaphore_signal(
                    met_sem.at[rounds], inc=1, device_id={"tp": tp_peer(k)}, device_id_type=MESH
                )

            loop(n_tp, tell)

    def all_met():
        @pl.when(me == 0)
        def _():
            pl.semaphore_wait(met_sem.at[rounds], n_tp - 1)

            def tell(k):
                pl.semaphore_signal(
                    met_sem.at[rounds + 1], inc=1, device_id={"sp": k}, device_id_type=MESH
                )

            loop(n_sp, tell)

    def round_end():
        pl.when(me > 0)(lambda: pl.semaphore_wait(met_sem.at[rounds + 1], 1))

    round_signal(0)
    loads[0].wait()
    loads[1].wait()

    in_order = [in_copy(t) for t in range(last)]
    ahead = min(1, last)

    @pl.when(has_prev)
    def _():
        for c in in_order[:ahead]:
            c.start()

    for c in loads[2:]:
        c.wait()
    q_gain = jnp.concatenate([q_gain_ref[...]] * 2, axis=1)
    k_gain = jnp.concatenate([k_gain_ref[...]] * 2, axis=1)
    low_lane = iota((TILE, LANES), 1) < LANES // 2

    def split_heads(x):
        first = jnp.where(low_lane, x, 0.0)
        second = jnp.where(low_lane, 0.0, x)
        return jnp.concatenate([first, second], axis=0).astype(jnp.bfloat16)

    def load_queries(q_from, g_from, t, q_to, g_to, unit_to, scale_to):
        for p in range(pairs):
            x = q_from[span(t), pair_lanes(p)].astype(jnp.float32)
            unit, scale = unit_of(x)
            unit_to[p, span(t)] = unit
            if scale_to is not None:
                scale_to[p, span(t)] = scale
            q_to[p, t] = split_heads(unit * q_gain)
            g_to[p, t] = split_heads(g_from[span(t), pair_lanes(p)].astype(jnp.float32))

    key_at = iota((TILE, WIDE), 0)
    query_at = iota((TILE, WIDE), 1) % TILE
    causal = query_at >= key_at
    far_bias = jnp.where((key_at // 64) >= (query_at // 64), 0.0, MASKED)

    edge_bias = far_bias + jnp.where(has_prev, 0.0, MASKED)

    for p in range(pairs):
        for t in range(tiles):
            x = k_ref[span(t), pair_lanes(p)].astype(jnp.float32)
            unit, scale = unit_of(x)
            k_unit[p, span(t)] = unit
            k_scale[p, span(t)] = scale
            hat = unit * k_gain
            k_hat[p, span(t)] = hat.astype(jnp.bfloat16)
            k_turned[p, :, span(t)] = hat.T.astype(jnp.bfloat16)
        sheets = []
        for h in (2 * p, 2 * p + 1):
            table = (bias_ref[h : h + 1, 0:CLIP] - bias_ref[h : h + 1, CLIP : CLIP + 1]) * LOG2E
            sheets.append(by_distance(table))
        near_bias[p] = jnp.concatenate(sheets, axis=1)
    dk[...] = jnp.zeros_like(dk)
    dv[...] = jnp.zeros_like(dv)
    taps[...] = jnp.zeros_like(taps)
    totals[...] = jnp.zeros_like(totals)
    gain_part[...] = jnp.zeros_like(gain_part)
    k_gain_part[...] = jnp.zeros_like(k_gain_part)

    def forward(p, t, start, stop, kinds, q_from, g_from, e_to, p_to):
        keys = slice(start * TILE, stop * TILE)
        raw = dot(k_hat[p, keys], q_from[p, t], NT)
        grad = dot(v_ref[keys, pair_lanes(p)], g_from[p, t], NT)
        total = jnp.zeros((1, WIDE), jnp.float32)
        inner = jnp.zeros((1, WIDE), jnp.float32)
        for c in range(start, stop):
            here = slice((c - start) * TILE, (c - start + 1) * TILE)
            s = raw[here] * (score_scale * LOG2E)
            kind = kinds.get(c)
            if kind == "diagonal":
                s = jnp.where(causal, s + near_bias[p], MASKED)
            elif kind == "below":
                s = s + jnp.where(causal, 0.0, near_bias[p])
            elif kind == "far":
                s = s + far_bias
            e = jnp.exp2(s)
            dp = grad[here]
            e_to[p, t, span(c)] = e
            p_to[p, t, span(c)] = dp
            total = total + jnp.sum(e, axis=0, keepdims=True)
            inner = inner + jnp.sum(e * dp, axis=0, keepdims=True)
        return total, inner

    def backward(p, t, start, stop, kinds, q_from, g_from, e_from, p_from, inverse, delta):
        keys = slice(start * TILE, stop * TILE)
        attention = e_from[p, t, keys] * inverse
        grad = attention * (p_from[p, t, keys] - delta)
        attention_low = attention.astype(jnp.bfloat16)
        grad_low = grad.astype(jnp.bfloat16)
        dv[p, keys] += dot(attention_low, g_from[p, t])
        dk[p, keys] += dot(grad_low, q_from[p, t])
        turned = dot(k_turned[p, :, keys], grad_low)
        totals[p : p + 1] += jnp.sum(grad, axis=0, keepdims=True)
        for c, kind in kinds.items():
            part = grad[(c - start) * TILE : (c - start + 1) * TILE]
            if kind == "diagonal":
                taps[p] += part
            elif kind == "below":
                taps[p] += jnp.where(causal, 0.0, part)
        return turned_back(turned)

    def turned_back(turned):
        upper = iota((LANES, TILE), 0) < LANES // 2
        return jnp.where(upper, turned[:, :TILE], turned[:, TILE:]).T

    def own_kinds(t):
        kinds = {t: "diagonal"}
        if t > 0:
            kinds[t - 1] = "below"
        return kinds

    def far_forward_kinds(t):
        kinds = {t: "far"}
        if t == 0:
            kinds[tiles - 1] = "below"
        return kinds

    def stat_row(p, t):
        return 2 * (t * pairs + p)

    def normalizers(p, t, own, far):
        row = stat_row(p, t)
        total = own[row : row + 1] + far[t, 2 * p : 2 * p + 1]
        inner = own[row + 1 : row + 2] + far[t, 2 * p + 1 : 2 * p + 2]
        inverse = 1.0 / total
        return inverse, inner * inverse

    for t in range(tiles):
        load_queries(q_ref, g_ref, t, own_q, own_g, q_unit, q_scale)
        for p in range(pairs):
            total, inner = forward(p, t, 0, t + 1, own_kinds(t), own_q, own_g, own_e, own_p)
            row = stat_row(p, t)
            own_stat[row : row + 1] = total
            own_stat[row + 1 : row + 2] = inner

    @pl.when(has_prev)
    def _():
        own_copy().start()
        for c in in_order[ahead:]:
            c.start()

    @pl.when(jnp.logical_not(has_prev))
    def _():
        stat_recv[...] = jnp.zeros_like(stat_recv)
        prev_kv[...] = jnp.zeros_like(prev_kv)
        dq_recv[...] = jnp.zeros_like(dq_recv)

    @pl.when(jnp.logical_not(has_next))
    def _():
        side_recv[...] = jnp.zeros_like(side_recv)

    meet(0)

    def far_forward(t):
        @pl.when(has_next)
        def _():
            in_copy(t).wait_recv()
            load_queries(next_q, next_g, t, far_q, far_g, next_unit, None)
            for p in range(pairs):
                total, inner = forward(
                    p, t, t, tiles, far_forward_kinds(t), far_q, far_g, far_e, far_p
                )
                stat_send[t, 2 * p : 2 * p + 1] = total
                stat_send[t, 2 * p + 1 : 2 * p + 2] = inner
            stat_copy(t).start()

    def far_backward(t):
        @pl.when(has_next)
        def _():
            if t == 0:
                own_copy().wait_recv()
            for p in range(pairs):
                inverse, delta = normalizers(p, t, next_stat, stat_send)
                part = backward(
                    p, t, t, tiles, far_forward_kinds(t), far_q, far_g, far_e, far_p, inverse, delta
                )
                dq_send[t, :, pair_lanes(p)] = part.astype(jnp.bfloat16)
                gain_part[...] += jnp.sum(part * next_unit[p, span(t)], axis=0, keepdims=True)

    def dq_start(ts):
        @pl.when(has_next)
        def _():
            for t in ts:
                dq_copy(t).start()

    def side_forward(t):
        @pl.when(has_prev)
        def _():
            kv_copy().wait_recv()

        for p in range(pairs):
            unit, _ = unit_of(prev_k[:, pair_lanes(p)].astype(jnp.float32))
            prev_unit[p] = unit
            hat = unit * k_gain
            prev_hat[p] = hat.astype(jnp.bfloat16)
            prev_turned[p] = hat.T.astype(jnp.bfloat16)
            raw = dot(prev_hat[p], own_q[p, t], NT)
            dp = dot(prev_v[:, pair_lanes(p)], own_g[p, t], NT)
            e = jnp.exp2(raw * (score_scale * LOG2E) + edge_bias)
            far_e[p, t, span(t)] = e
            far_p[p, t, span(t)] = dp
            stat_recv[t, 2 * p : 2 * p + 1] = jnp.sum(e, axis=0, keepdims=True)
            stat_recv[t, 2 * p + 1 : 2 * p + 2] = jnp.sum(e * dp, axis=0, keepdims=True)

    def side_backward(t):
        for p in range(pairs):
            inverse, delta = normalizers(p, t, own_stat, stat_recv)
            attention = far_e[p, t, span(t)] * inverse
            grad = attention * (far_p[p, t, span(t)] - delta)
            attention_low = attention.astype(jnp.bfloat16)
            grad_low = grad.astype(jnp.bfloat16)
            dk_part = dot(grad_low, own_q[p, t])
            side_send[0, :, pair_lanes(p)] = dk_part.astype(jnp.bfloat16)
            side_send[1, :, pair_lanes(p)] = dot(attention_low, own_g[p, t]).astype(jnp.bfloat16)
            k_gain_part[...] += jnp.sum(dk_part * prev_unit[p], axis=0, keepdims=True)
            totals[p : p + 1] += jnp.sum(grad, axis=0, keepdims=True)
            part = turned_back(dot(prev_turned[p], grad_low))
            dq_own[p, span(t)] += part
            gain_part[...] += jnp.sum(part * q_unit[p, span(t)], axis=0, keepdims=True)

    def kv_start():
        pl.when(has_next)(lambda: kv_copy().start())

    def side_start(odd):
        pl.when(has_prev & (lax.rem(me, 2) == odd))(lambda: side_copy().start())

    def own_backward(t):
        if t < last:

            @pl.when(has_prev)
            def _():
                stat_copy(t).wait_recv()

        for p in range(pairs):
            inverse, delta = normalizers(p, t, own_stat, stat_recv)
            part = backward(
                p, t, 0, t + 1, own_kinds(t), own_q, own_g, own_e, own_p, inverse, delta
            )
            dq_own[p, span(t)] = part
            gain_part[...] += jnp.sum(part * q_unit[p, span(t)], axis=0, keepdims=True)

    for t in range(last):
        far_forward(t)
        far_backward(t)
        if t == max(last - 2, 0):
            kv_start()
        if t < last - 1:
            meet(t + 1)
    for r in range(last, rounds):
        meet(r)
    column_met()
    early = max(last - 1, 0)
    for t in range(last - 1):
        own_backward(t)
    all_met()
    dq_start(range(early))
    side_forward(last)
    own_backward(last)
    side_backward(last)
    side_start(1)
    own_backward(last - 1)

    round_end()
    k_part = k_gain_part[...]
    for p in range(pairs):
        k_part = k_part + jnp.sum(dk[p] * k_unit[p], axis=0, keepdims=True)

    halves = [x + pltpu.roll(x, LANES // 2, 1) for x in (gain_part[...], k_part)]
    first_half = iota((1, LANES), 1) < LANES // 2
    gain_message[...] = jnp.where(first_half, halves[0], halves[1]) * score_scale

    def gain_copy(slot, target):
        return pltpu.make_async_remote_copy(
            src_ref=gain_message,
            dst_ref=gain_gathered.at[slot],
            send_sem=gain_send_sem.at[0],
            recv_sem=gain_recv_sem.at[0],
            device_id={"sp": target // n_tp, "tp": lax.rem(target, n_tp)},
            device_id_type=MESH,
        )

    def gain_start(k):
        gain_copy(me_flat, flat_peer(k)).start()

    if everyone <= 64:
        for k in range(1, everyone):
            gain_start(k)
    else:
        loop(everyone, gain_start)
    gain_gathered[me_flat] = gain_message[...]

    if message.shape[0] > 2 * heads:
        message[...] = jnp.zeros_like(message)
    for h in range(heads):
        lanes = slice((h % 2) * TILE, (h % 2 + 1) * TILE)
        row = distance_sums(taps[h // 2, :, lanes])
        rest = jnp.sum(totals[h // 2 : h // 2 + 1, lanes], axis=1, keepdims=True) - jnp.sum(
            row, axis=1, keepdims=True
        )
        message[h : h + 1] = row
        message[heads + h : heads + h + 1] = jnp.broadcast_to(rest, (1, LANES))

    def sum_copy(slot, target):
        return copy(message, gathered.at[slot], sum_send_sem.at[0], sum_recv_sem.at[0], target)

    loop(n_sp, lambda k: sum_copy(me, sp_peer(k)).start())
    gathered[me] = message[...]
    dq_start(range(early, last))
    side_start(0)

    def norm_backward(unit, scale, grad_hat, gain):
        grad_unit = grad_hat * gain
        inner = half_mean(grad_unit * unit)
        return (scale * (grad_unit - unit * inner)).astype(jnp.bfloat16)

    def finish_keys(t, dk_more, dv_more):
        for p in range(pairs):
            here = (p, span(t))
            dk_all, dv_all = dk[here], dv[here]
            if dk_more is not None:
                dk_all = dk_all + dk_more[:, pair_lanes(p)].astype(jnp.float32)
                dv_all = dv_all + dv_more[:, pair_lanes(p)].astype(jnp.float32)
            k_out[span(t), pair_lanes(p)] = norm_backward(
                k_unit[here], k_scale[here], dk_all * score_scale, k_gain
            )
            v_out[span(t), pair_lanes(p)] = dv_all.astype(jnp.bfloat16)

    def finish_queries(t, dq_more):
        for p in range(pairs):
            here = (p, span(t))
            dq_all = dq_own[here]
            if dq_more is not None:
                dq_all = dq_all + dq_more[:, pair_lanes(p)].astype(jnp.float32)
            q_out[span(t), pair_lanes(p)] = norm_backward(
                q_unit[here], q_scale[here], dq_all * score_scale, q_gain
            )

    for t in range(last):
        finish_keys(t, None, None)
    finish_queries(last, None)
    for t in range(last):

        @pl.when(has_prev)
        def _():
            dq_copy(t).wait_recv()

        finish_queries(t, dq_recv.at[t])

    @pl.when(has_next)
    def _():
        side_copy().wait_recv()

    finish_keys(last, side_recv.at[0], side_recv.at[1])
    def drain():
        @pl.when(has_prev)
        def _():
            own_copy().wait_send()
            side_copy().wait_send()
            for c in in_order:
                c.wait_send()

        @pl.when(has_next)
        def _():
            kv_copy().wait_send()
            for t in range(last):
                stat_copy(t).wait_send()
                dq_copy(t).wait_send()

    all_sums = gathered.at[0 : n_sp - 1]
    all_sums = copy(all_sums, all_sums, sum_send_sem.at[0], sum_recv_sem.at[0], before)
    all_gains = gain_gathered.at[0 : everyone - 1]
    all_gains = copy(all_gains, all_gains, gain_send_sem.at[0], gain_recv_sem.at[0], before)
    all_sums.wait_send()
    all_gains.wait_send()
    drain()
    all_sums.wait_recv()
    summed = jnp.sum(gathered[...], axis=0)
    for h in range(heads):
        bias_out[h : h + 1, 0:CLIP] = summed[h : h + 1]
        bias_out[h : h + 1, CLIP : CLIP + 1] = summed[heads + h : heads + h + 1, 0:1]
    all_gains.wait_recv()
    gains = jnp.sum(gain_gathered[...], axis=0)
    q_gain_out[...] = gains[:, 0 : LANES // 2]
    k_gain_out[...] = gains[:, LANES // 2 :]


def place(*refs):
    half = len(refs) // 2
    sem = refs[-1]
    moves = [
        pltpu.make_async_copy(source, target, sem.at[i])
        for i, (source, target) in enumerate(zip(refs[:half], refs[half:-1]))
    ]
    for c in moves:
        c.start()
    for c in moves:
        c.wait()


def per_device(axis_sizes, query, key, value, out_grad, query_gain, key_gain, rel_bias):
    n_sp, n_tp = axis_sizes
    rows, width = query.shape
    heads, taps = rel_bias.shape
    head_width = width // heads
    tiles = rows // TILE
    pairs = width // LANES
    low, full = jnp.bfloat16, jnp.float32
    message_rows = -(-2 * heads // 8) * 8
    stat_rows = -(-2 * pairs // 8) * 8
    vmem = pl.BlockSpec(memory_space=pltpu.VMEM)
    anywhere = pl.BlockSpec(memory_space=pl.ANY)
    stat = pltpu.VMEM((tiles, stat_rows, WIDE), full)
    sums = pltpu.VMEM((-(-2 * pairs * tiles // 8) * 8, WIDE), full)
    wide = pltpu.VMEM((pairs, tiles, WIDE, LANES), low)
    square = pltpu.VMEM((pairs, tiles, rows, WIDE), full)
    units = pltpu.VMEM((pairs, rows, LANES), full)
    dma = pltpu.SemaphoreType.DMA
    results = (
        ((rows, width), low),
        ((rows, width), low),
        ((rows, width), low),
        ((1, head_width), full),
        ((1, head_width), full),
        ((heads, taps), full),
    )
    given = (query, key, value, out_grad, query_gain.reshape(1, -1), key_gain.reshape(1, -1), rel_bias)
    kept = pl.pallas_call(
        functools.partial(kernel, axis_sizes, head_width),
        out_shape=tuple(pltpu.VMEM(shape, kind) for shape, kind in results),
        in_specs=[anywhere] * 7,
        out_specs=(vmem,) * 6,
        scratch_shapes=[pltpu.VMEM((2, rows, width), low)] * 2
        + [
            pltpu.VMEM((1, head_width), full),
            pltpu.VMEM((1, head_width), full),
            pltpu.VMEM((heads, taps), full),
        ]
        + [
            pltpu.VMEM((2, rows, width), low),
            pltpu.VMEM((2, TILE, width), low),
            pltpu.VMEM((pairs, TILE, LANES), low),
            pltpu.VMEM((pairs, LANES, TILE), low),
            pltpu.VMEM((pairs, TILE, LANES), full),
            pltpu.VMEM((2, TILE, width), low),
            pltpu.VMEM((2, TILE, width), low),
            pltpu.VMEM((1, LANES), full),
            stat,
            stat,
            sums,
            pltpu.VMEM((tiles, TILE, width), low),
            pltpu.VMEM((tiles, TILE, width), low),
            pltpu.VMEM((pairs, rows, LANES), low),
            pltpu.VMEM((pairs, LANES, rows), low),
            wide,
            wide,
            wide,
            wide,
            square,
            square,
            square,
            square,
            pltpu.VMEM((pairs, rows, LANES), full),
            pltpu.VMEM((pairs, rows, LANES), full),
            pltpu.VMEM((pairs, rows, LANES), full),
            pltpu.VMEM((pairs, TILE, WIDE), full),
            pltpu.VMEM((pairs, TILE, WIDE), full),
            pltpu.VMEM((8, WIDE), full),
            sums,
            units,
            units,
            units,
            units,
            units,
            pltpu.VMEM((1, LANES), full),
            pltpu.VMEM((message_rows, LANES), full),
            pltpu.VMEM((n_sp, message_rows, LANES), full),
            pltpu.VMEM((1, LANES), full),
            pltpu.VMEM((n_sp * n_tp, 1, LANES), full),
            dma((tiles,)),
            dma((tiles,)),
            dma((tiles,)),
            dma((tiles,)),
            dma((1,)),
            dma((1,)),
            dma((tiles,)),
            dma((tiles,)),
            dma((1,)),
            dma((1,)),
            dma((1,)),
            dma((1,)),
            dma((7,)),
            pltpu.SemaphoreType.REGULAR((max((n_sp - 1).bit_length(), 1) + 2,)),
            dma((1,)),
            dma((1,)),
            dma((1,)),
            dma((1,)),
        ],
        compiler_params=pltpu.CompilerParams(
            has_side_effects=True, collective_id=0, vmem_limit_bytes=MAIN_VMEM
        ),
    )(*(pltpu.with_memory_space_constraint(x, pltpu.HBM) for x in given))
    query_grad, key_grad, value_grad, query_gain_grad, key_gain_grad, bias_grad = pl.pallas_call(
        place,
        out_shape=tuple(jax.ShapeDtypeStruct(shape, kind) for shape, kind in results),
        in_specs=[vmem] * 6,
        out_specs=(anywhere,) * 6,
        scratch_shapes=[dma((6,))],
        compiler_params=pltpu.CompilerParams(vmem_limit_bytes=PLACE_VMEM),
    )(*kept)
    return (
        query_grad,
        key_grad,
        value_grad,
        query_gain_grad.reshape(-1),
        key_gain_grad.reshape(-1),
        bias_grad,
    )


def solution(mesh):
    axis_sizes = (mesh.shape["sp"], mesh.shape["tp"])
    placed = (P("sp", "tp"), P("sp", "tp"), P("sp", "tp"), P("sp", "tp"), P(), P(), P("tp", None))
    return jax.shard_map(
        functools.partial(per_device, axis_sizes),
        mesh=mesh,
        in_specs=placed,
        out_specs=(P("sp", "tp"), P("sp", "tp"), P("sp", "tp"), P(), P(), P("tp", None)),
        check_vma=False,
    )
```

```python
import functools

import jax
import jax.numpy as jnp
from jax import lax
from jax.experimental import pallas as pl
from jax.experimental.pallas import tpu as pltpu
from jax.sharding import PartitionSpec as P

CLIP = 128
TILE = 128
LANES = 128
WIDE = 2 * TILE
EPSILON = 1e-06
LOG2E = 1.4426950408889634
MASKED = -1e30
MAIN_VMEM = 48 * 1024 * 1024
PLACE_VMEM = 4 * 1024 * 1024
MESH = pl.DeviceIdType.MESH
NT = (((1,), (1,)), ((), ()))
NN = (((1,), (0,)), ((), ()))


def dot(a, b, dims=NN):
    return lax.dot_general(a, b, dims, preferred_element_type=jnp.float32)


def iota(shape, axis):
    return lax.broadcasted_iota(jnp.int32, shape, axis)


def half_mean(x):
    low = iota(x.shape, 1) < LANES // 2
    first = jnp.sum(jnp.where(low, x, 0.0), axis=1, keepdims=True)
    second = jnp.sum(jnp.where(low, 0.0, x), axis=1, keepdims=True)
    return jnp.where(low, first, second) * (2.0 / LANES)


def unit_of(x):
    scale = lax.rsqrt(half_mean(x * x) + EPSILON)
    return x * scale, scale


def low_skew(x, left):
    row = iota(x.shape, 0)
    for bit in range(3):
        step = 1 << bit
        moved = pltpu.roll(x, LANES - step if left else step, 1)
        x = jnp.where((row & step) != 0, moved, x)
    return x


def by_distance(table):
    first = low_skew(jnp.broadcast_to(table, (8, LANES)), False)
    blocks = [first] + [pltpu.roll(first, at, 1) for at in range(8, TILE, 8)]
    return jnp.concatenate(blocks, axis=0)


def distance_sums(x):
    total = x[0:8]
    for at in range(8, TILE, 8):
        total = total + pltpu.roll(x[at : at + 8], LANES - at, 1)
    return jnp.sum(low_skew(total, True), axis=0, keepdims=True)


def kernel(
    axis_sizes,
    head_width,
    q_hbm,
    k_hbm,
    v_hbm,
    g_hbm,
    q_gain_hbm,
    k_gain_hbm,
    bias_hbm,
    q_out,
    k_out,
    v_out,
    q_gain_out,
    k_gain_out,
    bias_out,
    qg_ref,
    kv_ref,
    q_gain_ref,
    k_gain_ref,
    bias_ref,
    next_qg,
    prev_kv,
    side_send,
    side_recv,
    stat_send,
    stat_recv,
    next_stat,
    dq_send,
    dq_recv,
    k_hat,
    k_turned,
    own_q,
    own_g,
    far_q,
    far_g,
    own_e,
    own_p,
    far_e,
    far_p,
    dk,
    dv,
    dq_own,
    near_bias,
    taps,
    totals,
    own_stat,
    q_unit,
    q_scale,
    next_unit,
    k_unit,
    k_scale,
    gain_part,
    message,
    gathered,
    gain_message,
    gain_gathered,
    in_send_sem,
    in_recv_sem,
    stat_send_sem,
    stat_recv_sem,
    own_send_sem,
    own_recv_sem,
    dq_send_sem,
    dq_recv_sem,
    sum_send_sem,
    sum_recv_sem,
    gain_send_sem,
    gain_recv_sem,
    load_sem,
    met_sem,
    kv_send_sem,
    kv_recv_sem,
    side_send_sem,
    side_recv_sem,
):
    n_sp, n_tp = axis_sizes
    rows, width = q_hbm.shape
    tiles = rows // TILE
    last = tiles - 1
    pairs = width // LANES
    heads = 2 * pairs
    score_scale = head_width ** (-0.5)
    me = lax.axis_index("sp")
    me_tp = lax.axis_index("tp")
    has_prev = me > 0
    has_next = me < n_sp - 1
    before = jnp.maximum(me - 1, 0)
    after = jnp.minimum(me + 1, n_sp - 1)

    q_ref, g_ref = qg_ref.at[0], qg_ref.at[1]
    k_ref, v_ref = kv_ref.at[0], kv_ref.at[1]
    next_q, next_g = next_qg.at[0], next_qg.at[1]
    prev_k, prev_v = prev_kv.at[0], prev_kv.at[1]

    def span(t):
        return slice(t * TILE, (t + 1) * TILE)

    def pair_lanes(p):
        return slice(p * LANES, (p + 1) * LANES)

    def copy(src, dst, send, recv, target):
        return pltpu.make_async_remote_copy(
            src_ref=src,
            dst_ref=dst,
            send_sem=send,
            recv_sem=recv,
            device_id={"sp": target},
            device_id_type=MESH,
        )

    def in_copy(t):
        return copy(
            qg_ref.at[:, span(t)], next_qg.at[:, span(t)], in_send_sem.at[t], in_recv_sem.at[t], before
        )

    def stat_copy(t):
        return copy(stat_send.at[t], stat_recv.at[t], stat_send_sem.at[t], stat_recv_sem.at[t], after)

    def own_copy():
        return copy(own_stat, next_stat, own_send_sem.at[0], own_recv_sem.at[0], before)

    def dq_copy(t):
        return copy(dq_send.at[t], dq_recv.at[t], dq_send_sem.at[t], dq_recv_sem.at[t], after)

    def kv_copy():
        return copy(kv_ref.at[:, span(last)], prev_kv, kv_send_sem.at[0], kv_recv_sem.at[0], after)

    def side_copy():
        return copy(side_send, side_recv, side_send_sem.at[0], side_recv_sem.at[0], before)

    def loop(count, body):
        def step(i, carry):
            body(i + 1)
            return carry

        lax.fori_loop(0, count - 1, step, 0)

    def sp_peer(k):
        return lax.rem(me + k, n_sp)

    def tp_peer(k):
        return lax.rem(me_tp + k, n_tp)

    everyone = n_sp * n_tp
    me_flat = me * n_tp + me_tp

    def flat_peer(k):
        return lax.rem(me_flat + k, everyone)

    barrier = pltpu.get_barrier_semaphore()

    def greet(target):
        pl.semaphore_signal(barrier, inc=1, device_id=target, device_id_type=MESH)

    pl.when(has_prev)(lambda: greet({"sp": before}))
    pl.when(has_next)(lambda: greet({"sp": after}))
    pl.when(me == 0)(lambda: loop(n_tp, lambda k: greet({"tp": tp_peer(k)})))
    moves = (
        (q_hbm, q_ref),
        (g_hbm, g_ref),
        (k_hbm, k_ref),
        (v_hbm, v_ref),
        (q_gain_hbm, q_gain_ref),
        (k_gain_hbm, k_gain_ref),
        (bias_hbm, bias_ref),
    )
    loads = [pltpu.make_async_copy(a, b, load_sem.at[i]) for i, (a, b) in enumerate(moves)]
    for c in loads:
        c.start()
    neighbours = has_prev.astype(jnp.int32) + has_next.astype(jnp.int32)
    pl.semaphore_wait(barrier, neighbours + jnp.where(me == 0, n_tp - 1, 0))
    rounds = met_sem.shape[0] - 2

    def round_signal(r):
        for ok, target in ((me >= 1 << r, me - (1 << r)), (me + (1 << r) < n_sp, me + (1 << r))):

            @pl.when(ok)
            def _():
                pl.semaphore_signal(
                    met_sem.at[r], inc=1, device_id={"sp": target}, device_id_type=MESH
                )

    def round_wait(r):
        count = (me >= 1 << r).astype(jnp.int32) + (me + (1 << r) < n_sp).astype(jnp.int32)
        pl.semaphore_wait(met_sem.at[r], count)

    def meet(r):
        if r < rounds:
            round_wait(r)
        if r + 1 < rounds:
            round_signal(r + 1)

    def column_met():
        @pl.when(me == 0)
        def _():
            def tell(k):
                pl.semaphore_signal(
                    met_sem.at[rounds], inc=1, device_id={"tp": tp_peer(k)}, device_id_type=MESH
                )

            loop(n_tp, tell)

    def all_met():
        @pl.when(me == 0)
        def _():
            pl.semaphore_wait(met_sem.at[rounds], n_tp - 1)

            def tell(k):
                pl.semaphore_signal(
                    met_sem.at[rounds + 1], inc=1, device_id={"sp": k}, device_id_type=MESH
                )

            loop(n_sp, tell)

    def round_end():
        pl.when(me > 0)(lambda: pl.semaphore_wait(met_sem.at[rounds + 1], 1))

    round_signal(0)
    loads[0].wait()
    loads[1].wait()

    in_order = [in_copy(t) for t in range(last)]
    ahead = min(1, last)

    @pl.when(has_prev)
    def _():
        for c in in_order[:ahead]:
            c.start()

    for c in loads[2:]:
        c.wait()
    q_gain = jnp.concatenate([q_gain_ref[...]] * 2, axis=1)
    k_gain = jnp.concatenate([k_gain_ref[...]] * 2, axis=1)
    low_lane = iota((TILE, LANES), 1) < LANES // 2

    def split_heads(x):
        first = jnp.where(low_lane, x, 0.0)
        second = jnp.where(low_lane, 0.0, x)
        return jnp.concatenate([first, second], axis=0).astype(jnp.bfloat16)

    def load_queries(q_from, g_from, t, q_to, g_to, unit_to, scale_to):
        for p in range(pairs):
            x = q_from[span(t), pair_lanes(p)].astype(jnp.float32)
            unit, scale = unit_of(x)
            unit_to[p, span(t)] = unit
            if scale_to is not None:
                scale_to[p, span(t)] = scale
            q_to[p, t] = split_heads(unit * q_gain)
            g_to[p, t] = split_heads(g_from[span(t), pair_lanes(p)].astype(jnp.float32))

    key_at = iota((TILE, WIDE), 0)
    query_at = iota((TILE, WIDE), 1) % TILE
    causal = query_at >= key_at
    far_bias = jnp.where((key_at // 64) >= (query_at // 64), 0.0, MASKED)

    edge_bias = far_bias + jnp.where(has_prev, 0.0, MASKED)

    for p in range(pairs):
        for t in range(tiles):
            x = k_ref[span(t), pair_lanes(p)].astype(jnp.float32)
            unit, scale = unit_of(x)
            k_unit[p, span(t)] = unit
            k_scale[p, span(t)] = scale
            hat = unit * k_gain
            k_hat[p, span(t)] = hat.astype(jnp.bfloat16)
            k_turned[p, :, span(t)] = hat.T.astype(jnp.bfloat16)
        sheets = []
        for h in (2 * p, 2 * p + 1):
            table = (bias_ref[h : h + 1, 0:CLIP] - bias_ref[h : h + 1, CLIP : CLIP + 1]) * LOG2E
            sheets.append(by_distance(table))
        near_bias[p] = jnp.concatenate(sheets, axis=1)
    dk[...] = jnp.zeros_like(dk)
    dv[...] = jnp.zeros_like(dv)
    taps[...] = jnp.zeros_like(taps)
    totals[...] = jnp.zeros_like(totals)
    gain_part[...] = jnp.zeros_like(gain_part)

    def forward(p, t, start, stop, kinds, q_from, g_from, e_to, p_to):
        keys = slice(start * TILE, stop * TILE)
        raw = dot(k_hat[p, keys], q_from[p, t], NT)
        grad = dot(v_ref[keys, pair_lanes(p)], g_from[p, t], NT)
        total = jnp.zeros((1, WIDE), jnp.float32)
        inner = jnp.zeros((1, WIDE), jnp.float32)
        for c in range(start, stop):
            here = slice((c - start) * TILE, (c - start + 1) * TILE)
            s = raw[here] * (score_scale * LOG2E)
            kind = kinds.get(c)
            if kind == "diagonal":
                s = jnp.where(causal, s + near_bias[p], MASKED)
            elif kind == "below":
                s = s + jnp.where(causal, 0.0, near_bias[p])
            elif kind == "far":
                s = s + far_bias
            e = jnp.exp2(s)
            dp = grad[here]
            e_to[p, t, span(c)] = e
            p_to[p, t, span(c)] = dp
            total = total + jnp.sum(e, axis=0, keepdims=True)
            inner = inner + jnp.sum(e * dp, axis=0, keepdims=True)
        return total, inner

    def backward(p, t, start, stop, kinds, q_from, g_from, e_from, p_from, inverse, delta):
        keys = slice(start * TILE, stop * TILE)
        attention = e_from[p, t, keys] * inverse
        grad = attention * (p_from[p, t, keys] - delta)
        attention_low = attention.astype(jnp.bfloat16)
        grad_low = grad.astype(jnp.bfloat16)
        dv[p, keys] += dot(attention_low, g_from[p, t])
        dk[p, keys] += dot(grad_low, q_from[p, t])
        turned = dot(k_turned[p, :, keys], grad_low)
        totals[p : p + 1] += jnp.sum(grad, axis=0, keepdims=True)
        for c, kind in kinds.items():
            part = grad[(c - start) * TILE : (c - start + 1) * TILE]
            if kind == "diagonal":
                taps[p] += part
            elif kind == "below":
                taps[p] += jnp.where(causal, 0.0, part)
        return turned_back(turned)

    def turned_back(turned):
        upper = iota((LANES, TILE), 0) < LANES // 2
        return jnp.where(upper, turned[:, :TILE], turned[:, TILE:]).T

    def own_kinds(t):
        kinds = {t: "diagonal"}
        if t > 0:
            kinds[t - 1] = "below"
        return kinds

    def far_forward_kinds(t):
        kinds = {t: "far"}
        if t == 0:
            kinds[tiles - 1] = "below"
        return kinds

    def stat_row(p, t):
        return 2 * (t * pairs + p)

    def normalizers(p, t, own, far):
        row = stat_row(p, t)
        total = own[row : row + 1] + far[t, 2 * p : 2 * p + 1]
        inner = own[row + 1 : row + 2] + far[t, 2 * p + 1 : 2 * p + 2]
        inverse = 1.0 / total
        return inverse, inner * inverse

    for t in range(tiles):
        load_queries(q_ref, g_ref, t, own_q, own_g, q_unit, q_scale)
        for p in range(pairs):
            total, inner = forward(p, t, 0, t + 1, own_kinds(t), own_q, own_g, own_e, own_p)
            row = stat_row(p, t)
            own_stat[row : row + 1] = total
            own_stat[row + 1 : row + 2] = inner

    @pl.when(has_prev)
    def _():
        own_copy().start()
        for c in in_order[ahead:]:
            c.start()

    @pl.when(jnp.logical_not(has_prev))
    def _():
        stat_recv[...] = jnp.zeros_like(stat_recv)
        prev_kv[...] = jnp.zeros_like(prev_kv)
        dq_recv[...] = jnp.zeros_like(dq_recv)

    @pl.when(jnp.logical_not(has_next))
    def _():
        side_recv[...] = jnp.zeros_like(side_recv)

    meet(0)

    def far_forward(t):
        @pl.when(has_next)
        def _():
            in_copy(t).wait_recv()
            load_queries(next_q, next_g, t, far_q, far_g, next_unit, None)
            for p in range(pairs):
                total, inner = forward(
                    p, t, t, tiles, far_forward_kinds(t), far_q, far_g, far_e, far_p
                )
                stat_send[t, 2 * p : 2 * p + 1] = total
                stat_send[t, 2 * p + 1 : 2 * p + 2] = inner
            stat_copy(t).start()

    def far_backward(t):
        @pl.when(has_next)
        def _():
            if t == 0:
                own_copy().wait_recv()
            for p in range(pairs):
                inverse, delta = normalizers(p, t, next_stat, stat_send)
                part = backward(
                    p, t, t, tiles, far_forward_kinds(t), far_q, far_g, far_e, far_p, inverse, delta
                )
                dq_send[t, :, pair_lanes(p)] = part.astype(jnp.bfloat16)
                gain_part[...] += jnp.sum(part * next_unit[p, span(t)], axis=0, keepdims=True)

    def dq_start(ts):
        @pl.when(has_next)
        def _():
            for t in ts:
                dq_copy(t).start()

    def side_forward(t):
        @pl.when(has_prev)
        def _():
            kv_copy().wait_recv()

        for p in range(pairs):
            unit, _ = unit_of(prev_k[:, pair_lanes(p)].astype(jnp.float32))
            k_unit[p, span(tiles)] = unit
            hat = unit * k_gain
            k_turned[p, :, span(tiles)] = hat.T.astype(jnp.bfloat16)
            raw = dot(hat.astype(jnp.bfloat16), own_q[p, t], NT)
            dp = dot(prev_v[:, pair_lanes(p)], own_g[p, t], NT)
            e = jnp.exp2(raw * (score_scale * LOG2E) + edge_bias)
            own_e[p, t, span(tiles)] = e
            own_p[p, t, span(tiles)] = dp
            stat_recv[t, 2 * p : 2 * p + 1] = jnp.sum(e, axis=0, keepdims=True)
            stat_recv[t, 2 * p + 1 : 2 * p + 2] = jnp.sum(e * dp, axis=0, keepdims=True)

    def side_pack():
        for p in range(pairs):
            side_send[0, :, pair_lanes(p)] = dk[p, span(tiles)].astype(jnp.bfloat16)
            side_send[1, :, pair_lanes(p)] = dv[p, span(tiles)].astype(jnp.bfloat16)

    def kv_start():
        pl.when(has_next)(lambda: kv_copy().start())

    def side_start(odd):
        pl.when(has_prev & (lax.rem(me, 2) == odd))(lambda: side_copy().start())

    def own_backward(t):
        if t < last:

            @pl.when(has_prev)
            def _():
                stat_copy(t).wait_recv()

        stop = t + 1 if t < last else tiles + 1
        for p in range(pairs):
            inverse, delta = normalizers(p, t, own_stat, stat_recv)
            part = backward(
                p, t, 0, stop, own_kinds(t), own_q, own_g, own_e, own_p, inverse, delta
            )
            dq_own[p, span(t)] = part
            gain_part[...] += jnp.sum(part * q_unit[p, span(t)], axis=0, keepdims=True)

    for t in range(last):
        far_forward(t)
        far_backward(t)
        if t == max(last - 2, 0):
            kv_start()
        if t < last - 1:
            meet(t + 1)
    for r in range(last, rounds):
        meet(r)
    column_met()
    early = max(last - 1, 0)
    for t in range(last - 1):
        own_backward(t)
    all_met()
    dq_start(range(early))
    side_forward(last)
    own_backward(last)
    side_pack()
    side_start(1)
    own_backward(last - 1)

    round_end()
    k_part = jnp.zeros((1, LANES), jnp.float32)
    for p in range(pairs):
        k_part = k_part + jnp.sum(dk[p] * k_unit[p], axis=0, keepdims=True)

    halves = [x + pltpu.roll(x, LANES // 2, 1) for x in (gain_part[...], k_part)]
    first_half = iota((1, LANES), 1) < LANES // 2
    gain_message[...] = jnp.where(first_half, halves[0], halves[1]) * score_scale

    def gain_copy(slot, target):
        return pltpu.make_async_remote_copy(
            src_ref=gain_message,
            dst_ref=gain_gathered.at[slot],
            send_sem=gain_send_sem.at[0],
            recv_sem=gain_recv_sem.at[0],
            device_id={"sp": target // n_tp, "tp": lax.rem(target, n_tp)},
            device_id_type=MESH,
        )

    def gain_start(k):
        gain_copy(me_flat, flat_peer(k)).start()

    if everyone <= 64:
        for k in range(1, everyone):
            gain_start(k)
    else:
        loop(everyone, gain_start)
    gain_gathered[me_flat] = gain_message[...]

    if message.shape[0] > 2 * heads:
        message[...] = jnp.zeros_like(message)
    for h in range(heads):
        lanes = slice((h % 2) * TILE, (h % 2 + 1) * TILE)
        row = distance_sums(taps[h // 2, :, lanes])
        rest = jnp.sum(totals[h // 2 : h // 2 + 1, lanes], axis=1, keepdims=True) - jnp.sum(
            row, axis=1, keepdims=True
        )
        message[h : h + 1] = row
        message[heads + h : heads + h + 1] = jnp.broadcast_to(rest, (1, LANES))

    def sum_copy(slot, target):
        return copy(message, gathered.at[slot], sum_send_sem.at[0], sum_recv_sem.at[0], target)

    loop(n_sp, lambda k: sum_copy(me, sp_peer(k)).start())
    gathered[me] = message[...]
    dq_start(range(early, last))
    side_start(0)

    def norm_backward(unit, scale, grad_hat, gain):
        grad_unit = grad_hat * gain
        inner = half_mean(grad_unit * unit)
        return (scale * (grad_unit - unit * inner)).astype(jnp.bfloat16)

    def finish_keys(t, dk_more, dv_more):
        for p in range(pairs):
            here = (p, span(t))
            dk_all, dv_all = dk[here], dv[here]
            if dk_more is not None:
                dk_all = dk_all + dk_more[:, pair_lanes(p)].astype(jnp.float32)
                dv_all = dv_all + dv_more[:, pair_lanes(p)].astype(jnp.float32)
            k_out[span(t), pair_lanes(p)] = norm_backward(
                k_unit[here], k_scale[here], dk_all * score_scale, k_gain
            )
            v_out[span(t), pair_lanes(p)] = dv_all.astype(jnp.bfloat16)

    def finish_queries(t, dq_more):
        for p in range(pairs):
            here = (p, span(t))
            dq_all = dq_own[here]
            if dq_more is not None:
                dq_all = dq_all + dq_more[:, pair_lanes(p)].astype(jnp.float32)
            q_out[span(t), pair_lanes(p)] = norm_backward(
                q_unit[here], q_scale[here], dq_all * score_scale, q_gain
            )

    for t in range(last):
        finish_keys(t, None, None)
    finish_queries(last, None)
    for t in range(last):

        @pl.when(has_prev)
        def _():
            dq_copy(t).wait_recv()

        finish_queries(t, dq_recv.at[t])

    @pl.when(has_next)
    def _():
        side_copy().wait_recv()

    finish_keys(last, side_recv.at[0], side_recv.at[1])
    def drain():
        @pl.when(has_prev)
        def _():
            own_copy().wait_send()
            side_copy().wait_send()
            for c in in_order:
                c.wait_send()

        @pl.when(has_next)
        def _():
            kv_copy().wait_send()
            for t in range(last):
                stat_copy(t).wait_send()
                dq_copy(t).wait_send()

    all_sums = gathered.at[0 : n_sp - 1]
    all_sums = copy(all_sums, all_sums, sum_send_sem.at[0], sum_recv_sem.at[0], before)
    all_gains = gain_gathered.at[0 : everyone - 1]
    all_gains = copy(all_gains, all_gains, gain_send_sem.at[0], gain_recv_sem.at[0], before)
    all_sums.wait_send()
    all_gains.wait_send()
    drain()
    all_sums.wait_recv()
    summed = jnp.sum(gathered[...], axis=0)
    for h in range(heads):
        bias_out[h : h + 1, 0:CLIP] = summed[h : h + 1]
        bias_out[h : h + 1, CLIP : CLIP + 1] = summed[heads + h : heads + h + 1, 0:1]
    all_gains.wait_recv()
    gains = jnp.sum(gain_gathered[...], axis=0)
    q_gain_out[...] = gains[:, 0 : LANES // 2]
    k_gain_out[...] = gains[:, LANES // 2 :]


def place(*refs):
    half = len(refs) // 2
    sem = refs[-1]
    moves = [
        pltpu.make_async_copy(source, target, sem.at[i])
        for i, (source, target) in enumerate(zip(refs[:half], refs[half:-1]))
    ]
    for c in moves:
        c.start()
    for c in moves:
        c.wait()


def per_device(axis_sizes, query, key, value, out_grad, query_gain, key_gain, rel_bias):
    n_sp, n_tp = axis_sizes
    rows, width = query.shape
    heads, taps = rel_bias.shape
    head_width = width // heads
    tiles = rows // TILE
    pairs = width // LANES
    low, full = jnp.bfloat16, jnp.float32
    message_rows = -(-2 * heads // 8) * 8
    stat_rows = -(-2 * pairs // 8) * 8
    vmem = pl.BlockSpec(memory_space=pltpu.VMEM)
    anywhere = pl.BlockSpec(memory_space=pl.ANY)
    stat = pltpu.VMEM((tiles, stat_rows, WIDE), full)
    sums = pltpu.VMEM((-(-2 * pairs * tiles // 8) * 8, WIDE), full)
    wide = pltpu.VMEM((pairs, tiles, WIDE, LANES), low)
    square = pltpu.VMEM((pairs, tiles, rows + TILE, WIDE), full)
    units = pltpu.VMEM((pairs, rows, LANES), full)
    more_units = pltpu.VMEM((pairs, rows + TILE, LANES), full)
    dma = pltpu.SemaphoreType.DMA
    results = (
        ((rows, width), low),
        ((rows, width), low),
        ((rows, width), low),
        ((1, head_width), full),
        ((1, head_width), full),
        ((heads, taps), full),
    )
    given = (query, key, value, out_grad, query_gain.reshape(1, -1), key_gain.reshape(1, -1), rel_bias)
    kept = pl.pallas_call(
        functools.partial(kernel, axis_sizes, head_width),
        out_shape=tuple(pltpu.VMEM(shape, kind) for shape, kind in results),
        in_specs=[anywhere] * 7,
        out_specs=(vmem,) * 6,
        scratch_shapes=[pltpu.VMEM((2, rows, width), low)] * 2
        + [
            pltpu.VMEM((1, head_width), full),
            pltpu.VMEM((1, head_width), full),
            pltpu.VMEM((heads, taps), full),
        ]
        + [
            pltpu.VMEM((2, rows, width), low),
            pltpu.VMEM((2, TILE, width), low),
            pltpu.VMEM((2, TILE, width), low),
            pltpu.VMEM((2, TILE, width), low),
            stat,
            stat,
            sums,
            pltpu.VMEM((tiles, TILE, width), low),
            pltpu.VMEM((tiles, TILE, width), low),
            pltpu.VMEM((pairs, rows, LANES), low),
            pltpu.VMEM((pairs, LANES, rows + TILE), low),
            wide,
            wide,
            wide,
            wide,
            square,
            square,
            square,
            square,
            more_units,
            more_units,
            units,
            pltpu.VMEM((pairs, TILE, WIDE), full),
            pltpu.VMEM((pairs, TILE, WIDE), full),
            pltpu.VMEM((8, WIDE), full),
            sums,
            units,
            units,
            units,
            more_units,
            units,
            pltpu.VMEM((1, LANES), full),
            pltpu.VMEM((message_rows, LANES), full),
            pltpu.VMEM((n_sp, message_rows, LANES), full),
            pltpu.VMEM((1, LANES), full),
            pltpu.VMEM((n_sp * n_tp, 1, LANES), full),
            dma((tiles,)),
            dma((tiles,)),
            dma((tiles,)),
            dma((tiles,)),
            dma((1,)),
            dma((1,)),
            dma((tiles,)),
            dma((tiles,)),
            dma((1,)),
            dma((1,)),
            dma((1,)),
            dma((1,)),
            dma((7,)),
            pltpu.SemaphoreType.REGULAR((max((n_sp - 1).bit_length(), 1) + 2,)),
            dma((1,)),
            dma((1,)),
            dma((1,)),
            dma((1,)),
        ],
        compiler_params=pltpu.CompilerParams(
            has_side_effects=True, collective_id=0, vmem_limit_bytes=MAIN_VMEM
        ),
    )(*(pltpu.with_memory_space_constraint(x, pltpu.HBM) for x in given))
    query_grad, key_grad, value_grad, query_gain_grad, key_gain_grad, bias_grad = pl.pallas_call(
        place,
        out_shape=tuple(jax.ShapeDtypeStruct(shape, kind) for shape, kind in results),
        in_specs=[vmem] * 6,
        out_specs=(anywhere,) * 6,
        scratch_shapes=[dma((6,))],
        compiler_params=pltpu.CompilerParams(vmem_limit_bytes=PLACE_VMEM),
    )(*kept)
    return (
        query_grad,
        key_grad,
        value_grad,
        query_gain_grad.reshape(-1),
        key_gain_grad.reshape(-1),
        bias_grad,
    )


def solution(mesh):
    axis_sizes = (mesh.shape["sp"], mesh.shape["tp"])
    placed = (P("sp", "tp"), P("sp", "tp"), P("sp", "tp"), P("sp", "tp"), P(), P(), P("tp", None))
    return jax.shard_map(
        functools.partial(per_device, axis_sizes),
        mesh=mesh,
        in_specs=placed,
        out_specs=(P("sp", "tp"), P("sp", "tp"), P("sp", "tp"), P(), P(), P("tp", None)),
        check_vma=False,
    )
```
